32 devices in a mesh: sp: 16 (over z, y, x), dp: 2 (over core).
Axes of the slice: x: 2, y: 2, z: 4, core: 2. Of those that a mesh axis runs over, the one named last changes fastest.
Arguments:
- val_input: bfloat16 [2048, 1536], P('sp', 'dp'), may hold values from -24 to 24, as said below
- gate_input: bfloat16 [2048, 1536], P('sp', 'dp'), may hold values from -8 to 8
- cotangent: bfloat16 [2048, 4096], P('sp'), may hold values from -6 to 6
- out_weight: bfloat16 [4096, 1536], P('sp', 'dp'), may hold values from -0.09375 to 0.09375
- conv_taps: float32 [31, 1536], P(None, 'dp'), may hold values from -1 to 1
- norm_gain: float32 [1536], P('dp'), may hold values from 0.1 to 1.9
Outputs:
- grad_val: bfloat16 [2048, 1536], P('sp', 'dp')
- grad_gate: bfloat16 [2048, 1536], P('sp', 'dp')
- grad_out_weight: float32 [4096, 1536], P('sp', 'dp')
- grad_taps: float32 [31, 1536], P(None, 'dp')
- grad_gain: float32 [1536], P('dp')
The draws below stay inside these ranges and needn't reach their ends.
Inputs may be any that keep to these rules, and one draw needn't show every extreme that they name: `val_input`: blocks of 64 channels and blocks of 32 tokens carry their own scales.
All inputs are finite; a program needn't handle non-finite values.
Results may differ from the reference program's by a relative error of at most 0.0063.
Values may be sent and summed in bfloat16 or wider, within the bound.
A program may use at most 64 MiB of HBM per device.

```python
import jax
import jax.numpy as jnp
from jax import lax

D = 4096
C = 1536
KERNEL = 31
TOKENS = 2048


def draw_val_input(key, part):
    first, second, third = jax.random.split(key, 3)
    base = jax.random.normal(first, (TOKENS, C), jnp.float32)
    block_scale = jnp.exp(jax.random.uniform(second, (C // 64,), jnp.float32, jnp.log(0.3), jnp.log(3.0)))
    time_scale = jnp.exp(jax.random.uniform(third, (TOKENS // 32,), jnp.float32, jnp.log(0.5), jnp.log(2.0)))
    values = base * jnp.repeat(block_scale, 64)[None, :] * jnp.repeat(time_scale, 32)[:, None]
    return jnp.clip(values, -24.0, 24.0).astype(jnp.bfloat16)


def with_spikes(values, rng, source, target, blocks, factor):
    owner, partner = [(jnp.arange(values.shape[position]) // (values.shape[position] // blocks)).reshape([-1 if axis == position else 1 for axis in range(values.ndim)]) for position in (source, target)]
    chosen = jax.random.permutation(rng, blocks)[partner]
    strong = (owner == chosen) | (owner == (partner + blocks // 2) % blocks)
    return jnp.where(strong, factor * values, values)


def shard_levels(own_key, dims, pieces, low, top_value):
    def one(dim, parts):
        draws = jax.random.uniform(jax.random.fold_in(jax.random.fold_in(own_key, 6), dim), (parts,), jnp.float32, low / len(pieces), top_value / len(pieces))
        return jnp.repeat(jnp.exp(draws), dims[dim] // parts).reshape((-1,) + (1,) * (len(dims) - dim - 1))

    factor_of = one(*pieces[0])
    for cut in pieces[1:]:
        factor_of = factor_of * one(*cut)
    return factor_of


def bell_draw(key, shape, scale, bound, shards=(), held_as=jnp.bfloat16):
    entries = scale * jax.random.normal(key, shape, jnp.float32)
    if shards:
        entries = entries * shard_levels(key, shape, shards, -0.22, 0.18)
    return jnp.clip(entries, -bound, bound).astype(held_as)


def gaussian_with(key, extent, scale, limit, pieces, heavy, kind=jnp.bfloat16):
    entries = scale * jax.random.normal(key, extent, jnp.float32)
    if pieces:
        entries = entries * shard_levels(key, extent, pieces, -0.22, 0.18)
    return jnp.clip(with_spikes(entries, jax.random.fold_in(key, 3), *heavy), -limit, limit).astype(kind)


def setup_inputs(seed: int = 0) -> dict:
    keys = jax.random.split(jax.random.key(seed), 7)
    return {
        "val_input": draw_val_input(jax.random.fold_in(keys[6], 71), 0),
        "gate_input": bell_draw(keys[1], (TOKENS, C), 1.5, 8.0, ((0, 16), (1, 2))),
        "cotangent": gaussian_with(keys[2], (TOKENS, D), 1.0, 6.0, ((0, 16),), (0, 1, 16, 2.0)),
        "out_weight": bell_draw(keys[3], (D, C), D ** -0.5, 0.09375, ((0, 16), (1, 2))),
        "conv_taps": bell_draw(keys[4], (KERNEL, C), KERNEL ** -0.5, 1.0, ((1, 2),), jnp.float32),
        "norm_gain": jnp.clip(1.0 + 0.18 * jax.random.normal(keys[5], (C,), jnp.float32), 0.1, 1.9),
    }


norm_floor = 0.25

def reference(val_input, gate_input, cotangent, out_weight, conv_taps, norm_gain):
    length = val_input.shape[0]
    sigma_gate = jax.nn.sigmoid(gate_input.astype(jnp.float32))
    mixed_in = (val_input.astype(jnp.float32) * sigma_gate).astype(jnp.bfloat16)
    padded_in = jnp.pad(lax.optimization_barrier(mixed_in).astype(jnp.float32), ((KERNEL - 1, 0), (0, 0)))
    conv_out = jnp.zeros((length, C), jnp.float32)
    for offset in range(KERNEL):
        conv_out = conv_out + conv_taps[offset][None, :] * padded_in[offset:offset + length]
    conv_rows = lax.optimization_barrier(conv_out.astype(jnp.bfloat16)).astype(jnp.float32)
    row_mean = lax.optimization_barrier(jnp.sum(conv_rows, 1, keepdims=True)) / C
    row_var = lax.optimization_barrier(jnp.sum(conv_rows * conv_rows, 1, keepdims=True)) / C - row_mean * row_mean
    inv_scale = lax.rsqrt(row_var + norm_floor)
    normed = (conv_rows - row_mean) * inv_scale
    act = normed * norm_gain[None, :]
    sigma_act = jax.nn.sigmoid(act)
    swished = (act * sigma_act).astype(jnp.bfloat16)
    grad_mix = jnp.dot(cotangent, out_weight, preferred_element_type=jnp.float32)
    grad_out_weight = lax.dot_general(cotangent, swished, (((0,), (0,)), ((), ())), preferred_element_type=jnp.float32)
    grad_act = grad_mix * sigma_act * (1.0 + act * (1.0 - sigma_act))
    grad_gain = lax.optimization_barrier(jnp.sum(grad_act * normed, 0))
    grad_norm = grad_act * norm_gain[None, :]
    first_sum = lax.optimization_barrier(jnp.sum(grad_norm, 1, keepdims=True)) / C
    second_sum = lax.optimization_barrier(jnp.sum(grad_norm * normed, 1, keepdims=True)) / C
    grad_conv = (inv_scale * (grad_norm - first_sum - normed * second_sum)).astype(jnp.bfloat16)
    grad_float = lax.optimization_barrier(grad_conv).astype(jnp.float32)
    padded_grad = jnp.pad(grad_float, ((0, KERNEL - 1), (0, 0)))
    grad_mixed = jnp.zeros((length, C), jnp.float32)
    tap_list = []
    for offset in range(KERNEL):
        back = KERNEL - 1 - offset
        grad_mixed = grad_mixed + conv_taps[offset][None, :] * padded_grad[back:back + length]
        tap_list.append(lax.optimization_barrier(jnp.sum(grad_float * padded_in[offset:offset + length], 0)))
    grad_taps = jnp.stack(tap_list, 0)
    grad_rows = lax.optimization_barrier(grad_mixed.astype(jnp.bfloat16)).astype(jnp.float32)
    grad_val = (grad_rows * sigma_gate).astype(jnp.bfloat16)
    grad_gate = (grad_rows * val_input.astype(jnp.float32) * sigma_gate * (1.0 - sigma_gate)).astype(jnp.bfloat16)
    return (grad_val, grad_gate, grad_out_weight, grad_taps, grad_gain)
```

```python
import functools

import jax
import jax.numpy as jnp
from jax import lax
from jax.experimental import pallas as pl
from jax.experimental.pallas import tpu as pltpu
from jax.sharding import PartitionSpec as P

norm_floor = 0.25
F32 = jnp.float32
BF16 = jnp.bfloat16
LOW = 4


def kernel(dims, val, gate, cot, w, taps, gain, gv, gg, gw, gt,
           pin, gcp, nrm, dact, cbuf, sgm, acc1, acc2, inv,
           hs1, hr1, hs2, hr2, cotg, wg, swg, own_mix, mixs, mixr, own_gw, gws, gwr,
           ps1, pr1, ps2, pr2, red, r1, r2, gts,
           h1, h2, cs, cr, fs, fr, ws, wr, p1s, p1r, p2s, p2r, ss, sr, ms, mr, gs, gr,
           t1s, t1r, t2s, t2r, t3s, t3r):
    a, b, dp = dims
    sp = a * b
    tokens, width = val.shape
    taps_n = taps.shape[0]
    channels = width * dp
    chunks, halo_len, tw = pin.shape
    halo = halo_len - tokens
    base = halo - (taps_n - 1)
    rows_w = w.shape[0]
    depth = cotg.shape[1]
    part_t = tokens // dp
    rows_r = red.shape[0] // a

    s = lax.axis_index("sp")
    c = lax.axis_index("dp")
    hi = s // a
    lo = lax.rem(s, a)

    def hi_peer(j):
        return (lax.rem(hi + j, b) * a + lo, c)

    def lo_peer(j):
        return (hi * a + lax.rem(lo + j, a), c)

    def dp_peer(j):
        return (s, lax.rem(c + j, dp))

    after = (lax.rem(s + 1, sp), c)
    before = (lax.rem(s + sp - 1, sp), c)

    def remote(src, dst, send, recv, to):
        return pltpu.make_async_remote_copy(
            src_ref=src, dst_ref=dst, send_sem=send, recv_sem=recv,
            device_id=to, device_id_type=pl.DeviceIdType.MESH)

    def lanes(i):
        if chunks == 1:
            return pl.ds(0, tw)
        return pl.ds(pl.multiple_of(i * tw, tw), tw)

    barrier = pltpu.get_barrier_semaphore()
    peers = ([after, before] + [hi_peer(j) for j in range(1, b)]
             + [lo_peer(j) for j in range(1, a)] + [dp_peer(j) for j in range(1, dp)])
    for peer in peers:
        pl.semaphore_signal(barrier, inc=1, device_id=peer, device_id_type=pl.DeviceIdType.MESH)

    @pl.loop(0, chunks)
    def _(i):
        at = lanes(i)
        sig = jax.nn.sigmoid(gate[:, at].astype(F32))
        sgm[i] = sig
        mixed = (val[:, at].astype(F32) * sig).astype(BF16)
        hs1[:, at] = mixed[tokens - halo:]
        pin[i, halo:, :] = mixed.astype(F32)

    pl.semaphore_wait(barrier, len(peers))

    sends = []
    halo1 = remote(hs1, hr1, h1.at[0], h1.at[1], after)
    halo1.start()
    my_rows = pl.ds(pl.multiple_of(c * part_t, part_t), part_t)
    cot_in = []
    for j in range(1, b):
        other = lax.rem(hi + j, b)
        copy = remote(cot.at[my_rows, pl.ds(pl.multiple_of(other * depth, 128), depth)],
                      cotg.at[pl.ds(pl.multiple_of(hi * tokens + c * part_t, part_t), part_t), :],
                      cs.at[j - 1], cr.at[j - 1], hi_peer(j))
        copy.start()
        cot_in.append(copy)
    w_in = []
    for j in range(1, a):
        copy = remote(w, wg.at[pl.ds(pl.multiple_of(lo * rows_w, rows_w), rows_w), :],
                      ws.at[j - 1], wr.at[j - 1], lo_peer(j))
        copy.start()
        w_in.append(copy)
    own_rows = pl.ds(pl.multiple_of(hi * tokens, tokens), tokens)
    cotg[own_rows, :] = cot[:, pl.ds(pl.multiple_of(hi * depth, 128), depth)]
    wg[pl.ds(pl.multiple_of(lo * rows_w, rows_w), rows_w), :] = w[...]
    sends += [halo1] + cot_in + w_in

    halo1.wait_recv()
    keep_first = (s > 0).astype(F32)
    acc1[...] = jnp.zeros_like(acc1)
    acc2[...] = jnp.zeros_like(acc2)

    @pl.loop(0, chunks)
    def _(i):
        at = lanes(i)
        pin[i, :halo, :] = hr1[:, at].astype(F32) * keep_first
        total = jnp.zeros((tokens, tw), F32)
        for k in range(taps_n):
            total = total + taps[k:k + 1, at] * pin[i, base + k:base + k + tokens, :]
        rounded = total.astype(BF16).astype(F32)
        cbuf[i] = rounded
        acc1[...] += rounded
        acc2[...] += rounded * rounded

    def share(buf, got, send, recv):
        buf[0] = jnp.broadcast_to(jnp.sum(acc1[...], 1, keepdims=True), (tokens, tw))
        buf[1] = jnp.broadcast_to(jnp.sum(acc2[...], 1, keepdims=True), (tokens, tw))
        copies = []
        for j in range(1, dp):
            copy = remote(buf, got.at[j - 1], send.at[j - 1], recv.at[j - 1], dp_peer(j))
            copy.start()
            copies.append(copy)
        return copies

    def gathered(buf, got, copies):
        for copy in copies:
            copy.wait_recv()
        for j in range(1, dp):
            buf_sum = got[j - 1]
            acc1[...] = (buf[0] if j == 1 else acc1[...]) + buf_sum[0]
            acc2[...] = (buf[1] if j == 1 else acc2[...]) + buf_sum[1]

    first = share(ps1, pr1, p1s, p1r)
    gathered(ps1, pr1, first)
    sends += first
    mean = acc1[...] / channels
    inv[...] = lax.rsqrt(acc2[...] / channels - mean * mean + norm_floor)
    acc1[...] = mean

    @pl.loop(0, chunks)
    def _(i):
        at = lanes(i)
        normed = (cbuf[i] - acc1[...]) * inv[...]
        act = normed * gain[:, at]
        sig = jax.nn.sigmoid(act)
        swg[own_rows, at] = (act * sig).astype(BF16)
        nrm[i] = normed
        dact[i] = sig * (1.0 + act * (1.0 - sig))

    sw_in = []
    for j in range(1, b):
        copy = remote(swg.at[own_rows, :], swg.at[own_rows, :], ss.at[j - 1], sr.at[j - 1], hi_peer(j))
        copy.start()
        sw_in.append(copy)
    sends += sw_in

    forwards = []
    for j in range(1, b):
        cot_in[j - 1].wait_recv()
        origin = lax.rem(hi + b - j, b)
        rows = cotg.at[pl.ds(pl.multiple_of(origin * tokens + c * part_t, part_t), part_t), :]
        for d in range(1, dp):
            copy = remote(rows, rows, fs.at[j - 1, d - 1], fr.at[j - 1, d - 1], dp_peer(d))
            copy.start()
            forwards.append(copy)
    for copy in w_in + forwards:
        copy.wait_recv()
    sends += forwards

    def mix_copy(j):
        return remote(mixs.at[j - 1], mixr.at[j - 1], ms.at[j - 1], mr.at[j - 1], hi_peer(j))

    @pl.loop(1, b)
    def _(j):
        other = lax.rem(hi + j, b)
        block = cotg[pl.ds(pl.multiple_of(other * tokens, tokens), tokens), :]
        mixs[j - 1] = jnp.dot(block, wg[...], preferred_element_type=F32).astype(BF16)
        mix_copy(j).start()

    own_mix[...] = jnp.dot(cotg[own_rows, :], wg[...], preferred_element_type=F32)

    for copy in sw_in:
        copy.wait_recv()

    def gw_copy(q, j):
        return remote(gws.at[q], gwr.at[j - 1], gs.at[j - 1], gr.at[j - 1], (hi * a + q, c))

    for q in range(a):
        part = lax.dot_general(cotg[:, q * rows_w:(q + 1) * rows_w], swg[...],
                               (((0,), (0,)), ((), ())), preferred_element_type=F32)

        @pl.when(lo == q)
        def _():
            own_gw[...] = part

        @pl.when(lo != q)
        def _():
            gws[q] = part.astype(BF16)
            gw_copy(q, lax.rem(q - lo + a, a)).start()

    for j in range(1, b):
        mix_copy(j).wait_recv()
    acc1[...] = jnp.zeros_like(acc1)
    acc2[...] = jnp.zeros_like(acc2)
    red[...] = jnp.zeros_like(red)

    @pl.loop(0, chunks)
    def _(i):
        at = lanes(i)
        mix = own_mix[:, at]
        for j in range(1, b):
            mix = mix + mixr[j - 1, :, at].astype(F32)
        grad_act = mix * dact[i]
        normed = nrm[i]
        red[taps_n:taps_n + 1, at] = jnp.sum(grad_act * normed, 0, keepdims=True)
        grad_norm = grad_act * gain[:, at]
        cbuf[i] = grad_norm
        acc1[...] += grad_norm
        acc2[...] += grad_norm * normed

    second = share(ps2, pr2, p2s, p2r)
    gathered(ps2, pr2, second)
    sends += second
    acc1[...] = acc1[...] / channels
    acc2[...] = acc2[...] / channels

    @pl.loop(0, chunks)
    def _(i):
        at = lanes(i)
        rounded = (inv[...] * (cbuf[i] - acc1[...] - nrm[i] * acc2[...])).astype(BF16)
        hs2[:, at] = rounded[:halo]
        gcp[i, :tokens, :] = rounded.astype(F32)

    halo2 = remote(hs2, hr2, h2.at[0], h2.at[1], before)
    halo2.start()
    sends.append(halo2)

    @pl.loop(0, chunks)
    def _(i):
        at = lanes(i)
        grad = gcp[i, :tokens, :]
        for k in range(taps_n):
            red[k:k + 1, at] = jnp.sum(grad * pin[i, base + k:base + k + tokens, :], 0, keepdims=True)

    stage1 = []
    for j in range(1, a):
        other = lax.rem(lo + j, a)
        copy = remote(red.at[pl.ds(pl.multiple_of(other * rows_r, 8), rows_r), :], r1.at[j - 1],
                      t1s.at[j - 1], t1r.at[j - 1], lo_peer(j))
        copy.start()
        stage1.append(copy)
    sends += stage1

    halo2.wait_recv()
    keep_last = (s < sp - 1).astype(F32)

    @pl.loop(0, chunks)
    def _(i):
        at = lanes(i)
        gcp[i, tokens:, :] = hr2[:, at].astype(F32) * keep_last
        total = jnp.zeros((tokens, tw), F32)
        for k in range(taps_n):
            back = taps_n - 1 - k
            total = total + taps[k:k + 1, at] * gcp[i, back:back + tokens, :]
        grad = total.astype(BF16).astype(F32)
        sig = sgm[i]
        gv[:, at] = (grad * sig).astype(BF16)
        gg[:, at] = (grad * val[:, at].astype(F32) * sig * (1.0 - sig)).astype(BF16)

    for copy in stage1:
        copy.wait_recv()
    mine = red[pl.ds(pl.multiple_of(lo * rows_r, 8), rows_r), :]
    for j in range(1, a):
        mine = mine + r1[j - 1]
    r2[hi] = mine
    stage2 = []
    for j in range(1, b):
        copy = remote(r2.at[hi], r2.at[hi], t2s.at[j - 1], t2r.at[j - 1], hi_peer(j))
        copy.start()
        stage2.append(copy)
    sends += stage2
    for copy in stage2:
        copy.wait_recv()
    summed = r2[0]
    for j in range(1, b):
        summed = summed + r2[j]
    my_red = pl.ds(pl.multiple_of(lo * rows_r, 8), rows_r)
    gts[my_red, :] = summed
    stage3 = []
    for j in range(1, a):
        copy = remote(gts.at[my_red, :], gts.at[my_red, :], t3s.at[j - 1], t3r.at[j - 1], lo_peer(j))
        copy.start()
        stage3.append(copy)
    sends += stage3

    for j in range(1, a):
        gw_copy(0, j).wait_recv()
    total = own_gw[...]
    for j in range(1, a):
        total = total + gwr[j - 1].astype(F32)
    gw[...] = total

    for copy in stage3:
        copy.wait_recv()
    gt[...] = gts[...]

    for copy in sends:
        copy.wait_send()
    for j in range(1, b):
        mix_copy(j).wait_send()
    for j in range(1, a):
        gw_copy(0, j).wait_send()


def body(sp, dp, val, gate, cot, w, taps, gain):
    a = LOW if sp % LOW == 0 else 1
    b = sp // a
    tokens, width = val.shape
    rows_w = w.shape[0]
    model = cot.shape[1]
    depth = model // b
    taps_n = taps.shape[0]
    tw = 128 if width % 128 == 0 else width
    chunks = width // tw
    halo = -(-(taps_n - 1) // 16) * 16
    rows = -(-(taps_n + 1) // (8 * a)) * 8 * a
    vm, dma = pltpu.VMEM, pltpu.SemaphoreType.DMA
    scratch = [
        vm((chunks, tokens + halo, tw), F32),
        vm((chunks, tokens + halo, tw), F32),
        vm((chunks, tokens, tw), F32),
        vm((chunks, tokens, tw), F32),
        vm((chunks, tokens, tw), F32),
        vm((chunks, tokens, tw), F32),
        vm((tokens, tw), F32),
        vm((tokens, tw), F32),
        vm((tokens, tw), F32),
        vm((halo, width), BF16),
        vm((halo, width), BF16),
        vm((halo, width), BF16),
        vm((halo, width), BF16),
        vm((b * tokens, depth), BF16),
        vm((depth, width), BF16),
        vm((b * tokens, width), BF16),
        vm((tokens, width), F32),
        vm((b - 1, tokens, width), BF16),
        vm((b - 1, tokens, width), BF16),
        vm((rows_w, width), F32),
        vm((a, rows_w, width), BF16),
        vm((a - 1, rows_w, width), BF16),
        vm((2, tokens, tw), F32),
        vm((dp - 1, 2, tokens, tw), F32),
        vm((2, tokens, tw), F32),
        vm((dp - 1, 2, tokens, tw), F32),
        vm((rows, width), F32),
        vm((a - 1, rows // a, width), F32),
        vm((b, rows // a, width), F32),
        vm((rows, width), F32),
        dma((2,)), dma((2,)),
        dma((b - 1,)), dma((b - 1,)),
        dma((b - 1, dp - 1)), dma((b - 1, dp - 1)),
        dma((a - 1,)), dma((a - 1,)),
        dma((dp - 1,)), dma((dp - 1,)), dma((dp - 1,)), dma((dp - 1,)),
        dma((b - 1,)), dma((b - 1,)),
        dma((b - 1,)), dma((b - 1,)),
        dma((a - 1,)), dma((a - 1,)),
        dma((a - 1,)), dma((a - 1,)),
        dma((b - 1,)), dma((b - 1,)),
        dma((a - 1,)), dma((a - 1,)),
    ]
    spec = pl.BlockSpec(memory_space=pltpu.VMEM)
    gv, gg, gw, gt = pl.pallas_call(
        functools.partial(kernel, (a, b, dp)),
        out_shape=(
            jax.ShapeDtypeStruct((tokens, width), BF16),
            jax.ShapeDtypeStruct((tokens, width), BF16),
            jax.ShapeDtypeStruct((rows_w, width), F32),
            jax.ShapeDtypeStruct((rows, width), F32),
        ),
        in_specs=[spec] * 6,
        out_specs=(spec,) * 4,
        scratch_shapes=scratch,
        compiler_params=pltpu.CompilerParams(
            collective_id=0, has_side_effects=True, vmem_limit_bytes=56 * 1024 * 1024),
    )(val, gate, cot, w, taps, gain[None, :])
    return gv, gg, gw, gt[:taps_n], gt[taps_n]


def solution(mesh):
    in_specs = (P("sp", "dp"), P("sp", "dp"), P("sp", None), P("sp", "dp"), P(None, "dp"), P("dp"))
    out_specs = (P("sp", "dp"), P("sp", "dp"), P("sp", "dp"), P(None, "dp"), P("dp"))
    run = functools.partial(body, mesh.shape["sp"], mesh.shape["dp"])
    return jax.shard_map(run, mesh=mesh, in_specs=in_specs, out_specs=out_specs, check_vma=False)
```

```python
import functools

import jax
import jax.numpy as jnp
from jax import lax
from jax.experimental import pallas as pl
from jax.experimental.pallas import tpu as pltpu
from jax.sharding import PartitionSpec as P

norm_floor = 0.25
F32 = jnp.float32
BF16 = jnp.bfloat16
LOW = 4


def kernel(dims, val_in, gate_in, cot, w, taps, gain, gv, gg, gw, gt,
           val, gate, loads, cott, pin, gcp, nrm, dact, cbuf, sgm, acc1, acc2, inv,
           hs1, hr1, hs2, hr2, cotg, wg, swg, own_mix, mixs, mixr, own_gw, gws, gwr,
           ps1, pr1, ps2, pr2, red, r1, r2, gts,
           h1, h2, cs, cr, fs, fr, ws, wr, p1s, p1r, p2s, p2r, ss, sr, ms, mr, gs, gr,
           t1s, t1r, t2s, t2r, t3s, t3r):
    a, b, dp = dims
    sp = a * b
    tokens, width = val.shape
    taps_n = taps.shape[0]
    channels = width * dp
    chunks, halo_len, tw = pin.shape
    halo = halo_len - tokens
    base = halo - (taps_n - 1)
    rows_w = w.shape[0]
    depth = cotg.shape[1]
    parts, _, wp = wg.shape
    per = chunks // parts
    part_t = tokens // dp
    rows_r = red.shape[0] // a

    s = lax.axis_index("sp")
    c = lax.axis_index("dp")
    hi = s // a
    lo = lax.rem(s, a)

    def hi_peer(j):
        return (lax.rem(hi + j, b) * a + lo, c)

    def lo_peer(j):
        return (hi * a + lax.rem(lo + j, a), c)

    def dp_peer(j):
        return (s, lax.rem(c + j, dp))

    after = (lax.rem(s + 1, sp), c)
    before = (lax.rem(s + sp - 1, sp), c)

    def remote(src, dst, send, recv, to):
        return pltpu.make_async_remote_copy(
            src_ref=src, dst_ref=dst, send_sem=send, recv_sem=recv,
            device_id=to, device_id_type=pl.DeviceIdType.MESH)

    def lanes(i):
        if chunks == 1:
            return pl.ds(0, tw)
        return pl.ds(pl.multiple_of(i * tw, tw), tw)

    def place(i):
        if parts == 1:
            return 0, lanes(i)
        return i // per, pl.ds(pl.multiple_of(lax.rem(i, per) * tw, tw), tw)

    own_rows = pl.ds(pl.multiple_of(hi * tokens, tokens), tokens)
    own_depth = pl.ds(pl.multiple_of(lo * rows_w, rows_w), rows_w)
    barrier = pltpu.get_barrier_semaphore()
    peers = ([after, before] + [hi_peer(j) for j in range(1, b)]
             + [lo_peer(j) for j in range(1, a)] + [dp_peer(j) for j in range(1, dp)])
    for peer in peers:
        pl.semaphore_signal(barrier, inc=1, device_id=peer, device_id_type=pl.DeviceIdType.MESH)

    local = [pltpu.make_async_copy(val_in, val, loads.at[0]),
             pltpu.make_async_copy(gate_in, gate, loads.at[1]),
             pltpu.make_async_copy(cot.at[:, pl.ds(pl.multiple_of(hi * depth, 128), depth)],
                                   cotg.at[own_rows, :], loads.at[2])]
    for h in range(parts):
        local.append(pltpu.make_async_copy(w.at[:, h * wp:(h + 1) * wp], wg.at[h, own_depth, :], loads.at[3 + h]))
    for copy in local:
        copy.start()
    local[0].wait()
    local[1].wait()

    @pl.loop(0, chunks)
    def _(i):
        at = lanes(i)
        sig = jax.nn.sigmoid(gate[:, at].astype(F32))
        sgm[i] = sig
        mixed = (val[:, at].astype(F32) * sig).astype(BF16)
        hs1[:, at] = mixed[tokens - halo:]
        pin[i, halo:, :] = mixed.astype(F32)

    pl.semaphore_wait(barrier, len(peers))

    sends = []
    halo1 = remote(hs1, hr1, h1.at[0], h1.at[1], after)
    halo1.start()
    my_rows = pl.ds(pl.multiple_of(c * part_t, part_t), part_t)
    cot_in = []
    for j in range(1, b):
        other = lax.rem(hi + j, b)
        copy = remote(cot.at[my_rows, pl.ds(pl.multiple_of(other * depth, 128), depth)],
                      cotg.at[pl.ds(pl.multiple_of(hi * tokens + c * part_t, part_t), part_t), :],
                      cs.at[j - 1], cr.at[j - 1], hi_peer(j))
        copy.start()
        cot_in.append(copy)
    w_in = [[] for _ in range(parts)]
    for h in range(parts):
        for j in range(1, a):
            copy = remote(w.at[:, h * wp:(h + 1) * wp], wg.at[h, own_depth, :],
                          ws.at[h, j - 1], wr.at[h, j - 1], lo_peer(j))
            copy.start()
            w_in[h].append(copy)
    sends += [halo1] + cot_in + sum(w_in, [])

    halo1.wait_recv()
    keep_first = (s > 0).astype(F32)
    acc1[...] = jnp.zeros_like(acc1)
    acc2[...] = jnp.zeros_like(acc2)

    @pl.loop(0, chunks)
    def _(i):
        at = lanes(i)
        pin[i, :halo, :] = hr1[:, at].astype(F32) * keep_first
        total = jnp.zeros((tokens, tw), F32)
        for k in range(taps_n):
            total = total + taps[k:k + 1, at] * pin[i, base + k:base + k + tokens, :]
        rounded = total.astype(BF16).astype(F32)
        cbuf[i] = rounded
        acc1[...] += rounded
        acc2[...] += rounded * rounded

    def share(buf, got, send, recv):
        buf[0] = jnp.broadcast_to(jnp.sum(acc1[...], 1, keepdims=True), (tokens, tw))
        buf[1] = jnp.broadcast_to(jnp.sum(acc2[...], 1, keepdims=True), (tokens, tw))
        copies = []
        for j in range(1, dp):
            copy = remote(buf, got.at[j - 1], send.at[j - 1], recv.at[j - 1], dp_peer(j))
            copy.start()
            copies.append(copy)
        return copies

    def gathered(buf, got, copies):
        for copy in copies:
            copy.wait_recv()
        for j in range(1, dp):
            buf_sum = got[j - 1]
            acc1[...] = (buf[0] if j == 1 else acc1[...]) + buf_sum[0]
            acc2[...] = (buf[1] if j == 1 else acc2[...]) + buf_sum[1]

    first = share(ps1, pr1, p1s, p1r)
    gathered(ps1, pr1, first)
    sends += first
    mean = acc1[...] / channels
    inv[...] = lax.rsqrt(acc2[...] / channels - mean * mean + norm_floor)
    acc1[...] = mean

    @pl.loop(0, chunks)
    def _(i):
        at = lanes(i)
        normed = (cbuf[i] - acc1[...]) * inv[...]
        act = normed * gain[at][None, :]
        part, within = place(i)
        sig = jax.nn.sigmoid(act)
        swg[part, own_rows, within] = (act * sig).astype(BF16)
        nrm[i] = normed
        dact[i] = sig * (1.0 + act * (1.0 - sig))

    def sw_copy(h, j):
        return remote(swg.at[h, own_rows, :], swg.at[h, own_rows, :],
                      ss.at[h, j - 1], sr.at[h, j - 1], hi_peer(j))

    for j in range(1, b):
        sw_copy(0, j).start()

    forwards = []
    for j in range(1, b):
        cot_in[j - 1].wait_recv()
        origin = lax.rem(hi + b - j, b)
        rows = cotg.at[pl.ds(pl.multiple_of(origin * tokens + c * part_t, part_t), part_t), :]
        for d in range(1, dp):
            copy = remote(rows, rows, fs.at[j - 1, d - 1], fr.at[j - 1, d - 1], dp_peer(d))
            copy.start()
            forwards.append(copy)
    sends += forwards
    for copy in local[2:]:
        copy.wait()
    for copy in forwards:
        copy.wait_recv()

    def mix_copy(h, j):
        return remote(mixs.at[h, j - 1], mixr.at[h, j - 1], ms.at[h, j - 1], mr.at[h, j - 1], hi_peer(j))

    for h in range(parts):
        for copy in w_in[h]:
            copy.wait_recv()

        @pl.loop(1, b)
        def _(j):
            other = lax.rem(hi + j, b)
            block = cotg[pl.ds(pl.multiple_of(other * tokens, tokens), tokens), :]
            mixs[h, j - 1] = jnp.dot(block, wg[h], preferred_element_type=F32).astype(BF16)
            mix_copy(h, j).start()

    for h in range(1, parts):
        for j in range(1, b):
            sw_copy(h, j).start()

    for h in range(parts):
        own_mix[h] = jnp.dot(cotg[own_rows, :], wg[h], preferred_element_type=F32)
    for q in range(a):
        cott[q * rows_w:(q + 1) * rows_w, :] = cotg[:, q * rows_w:(q + 1) * rows_w].T

    def gw_copy(h, j):
        return remote(gws.at[h, j - 1], gwr.at[h, j - 1], gs.at[h, j - 1], gr.at[h, j - 1], lo_peer(j))

    def gw_part(h):
        for j in range(1, b):
            sw_copy(h, j).wait_recv()

        @pl.loop(1, a)
        def _(j):
            other = lax.rem(lo + j, a)
            block = cott[pl.ds(pl.multiple_of(other * rows_w, rows_w), rows_w), :]
            gws[h, j - 1] = jnp.dot(block, swg[h], preferred_element_type=F32).astype(BF16)
            gw_copy(h, j).start()

        own_gw[h] = jnp.dot(cott[own_depth, :], swg[h], preferred_element_type=F32)

    gw_part(0)

    for h in range(parts):
        for j in range(1, b):
            mix_copy(h, j).wait_recv()
    acc1[...] = jnp.zeros_like(acc1)
    acc2[...] = jnp.zeros_like(acc2)
    red[...] = jnp.zeros_like(red)

    @pl.loop(0, chunks)
    def _(i):
        at = lanes(i)
        part, within = place(i)
        mix = own_mix[part, :, within]
        for j in range(1, b):
            mix = mix + mixr[part, j - 1, :, within].astype(F32)
        grad_act = mix * dact[i]
        normed = nrm[i]
        red[taps_n:taps_n + 1, at] = jnp.sum(grad_act * normed, 0, keepdims=True)
        grad_norm = grad_act * gain[at][None, :]
        cbuf[i] = grad_norm
        acc1[...] += grad_norm
        acc2[...] += grad_norm * normed

    second = share(ps2, pr2, p2s, p2r)
    gathered(ps2, pr2, second)
    sends += second
    acc1[...] = acc1[...] / channels
    acc2[...] = acc2[...] / channels

    @pl.loop(0, chunks)
    def _(i):
        at = lanes(i)
        rounded = (inv[...] * (cbuf[i] - acc1[...] - nrm[i] * acc2[...])).astype(BF16)
        hs2[:, at] = rounded[:halo]
        gcp[i, :tokens, :] = rounded.astype(F32)

    halo2 = remote(hs2, hr2, h2.at[0], h2.at[1], before)
    halo2.start()
    sends.append(halo2)

    @pl.loop(0, chunks)
    def _(i):
        at = lanes(i)
        grad = gcp[i, :tokens, :]
        for k in range(taps_n):
            red[k:k + 1, at] = jnp.sum(grad * pin[i, base + k:base + k + tokens, :], 0, keepdims=True)

    stage1 = []
    for j in range(1, a):
        other = lax.rem(lo + j, a)
        copy = remote(red.at[pl.ds(pl.multiple_of(other * rows_r, 8), rows_r), :], r1.at[j - 1],
                      t1s.at[j - 1], t1r.at[j - 1], lo_peer(j))
        copy.start()
        stage1.append(copy)
    sends += stage1
    for h in range(1, parts - 1):
        gw_part(h)

    halo2.wait_recv()
    keep_last = (s < sp - 1).astype(F32)

    @pl.loop(0, chunks)
    def _(i):
        at = lanes(i)
        gcp[i, tokens:, :] = hr2[:, at].astype(F32) * keep_last
        total = jnp.zeros((tokens, tw), F32)
        for k in range(taps_n):
            back = taps_n - 1 - k
            total = total + taps[k:k + 1, at] * gcp[i, back:back + tokens, :]
        grad = total.astype(BF16).astype(F32)
        sig = sgm[i]
        gv[:, at] = (grad * sig).astype(BF16)
        gg[:, at] = (grad * val[:, at].astype(F32) * sig * (1.0 - sig)).astype(BF16)

    for copy in stage1:
        copy.wait_recv()
    mine = red[pl.ds(pl.multiple_of(lo * rows_r, 8), rows_r), :]
    for j in range(1, a):
        mine = mine + r1[j - 1]
    r2[hi] = mine
    stage2 = []
    for j in range(1, b):
        copy = remote(r2.at[hi], r2.at[hi], t2s.at[j - 1], t2r.at[j - 1], hi_peer(j))
        copy.start()
        stage2.append(copy)
    sends += stage2
    if parts > 1:
        gw_part(parts - 1)
    for copy in stage2:
        copy.wait_recv()
    summed = r2[0]
    for j in range(1, b):
        summed = summed + r2[j]
    my_red = pl.ds(pl.multiple_of(lo * rows_r, 8), rows_r)
    gts[my_red, :] = summed
    stage3 = []
    for j in range(1, a):
        copy = remote(gts.at[my_red, :], gts.at[my_red, :], t3s.at[j - 1], t3r.at[j - 1], lo_peer(j))
        copy.start()
        stage3.append(copy)
    sends += stage3

    for h in range(parts):
        for j in range(1, a):
            gw_copy(h, j).wait_recv()
        total = own_gw[h]
        for j in range(1, a):
            total = total + gwr[h, j - 1].astype(F32)
        gw[:, h * wp:(h + 1) * wp] = total

    for copy in stage3:
        copy.wait_recv()
    gt[...] = gts[...]

    for copy in sends:
        copy.wait_send()
    for h in range(parts):
        for j in range(1, b):
            sw_copy(h, j).wait_send()
            mix_copy(h, j).wait_send()
        for j in range(1, a):
            gw_copy(h, j).wait_send()


def finish(gv, gg, gw, gt, out_gv, out_gg, out_gw, out_taps, out_gain):
    out_gv[...] = gv[...]
    out_gg[...] = gg[...]
    out_gw[...] = gw[...]
    taps_n = out_taps.shape[0]
    out_taps[...] = gt[:taps_n]
    out_gain[...] = gt[taps_n]


def body(sp, dp, val, gate, cot, w, taps, gain):
    a = LOW if sp % LOW == 0 else 1
    b = sp // a
    tokens, width = val.shape
    rows_w = w.shape[0]
    model = cot.shape[1]
    depth = model // b
    taps_n = taps.shape[0]
    tw = 128 if width % 128 == 0 else width
    chunks = width // tw
    halo = -(-(taps_n - 1) // 16) * 16
    rows = -(-(taps_n + 1) // (8 * a)) * 8 * a
    parts = 3 if chunks % 3 == 0 else 2 if chunks % 2 == 0 else 1
    wp = width // parts
    vm, dma = pltpu.VMEM, pltpu.SemaphoreType.DMA
    scratch = [
        vm((tokens, width), BF16),
        vm((tokens, width), BF16),
        dma((3 + parts,)),
        vm((depth, b * tokens), BF16),
        vm((chunks, tokens + halo, tw), F32),
        vm((chunks, tokens + halo, tw), F32),
        vm((chunks, tokens, tw), F32),
        vm((chunks, tokens, tw), F32),
        vm((chunks, tokens, tw), F32),
        vm((chunks, tokens, tw), F32),
        vm((tokens, tw), F32),
        vm((tokens, tw), F32),
        vm((tokens, tw), F32),
        vm((halo, width), BF16),
        vm((halo, width), BF16),
        vm((halo, width), BF16),
        vm((halo, width), BF16),
        vm((b * tokens, depth), BF16),
        vm((parts, depth, wp), BF16),
        vm((parts, b * tokens, wp), BF16),
        vm((parts, tokens, wp), F32),
        vm((parts, b - 1, tokens, wp), BF16),
        vm((parts, b - 1, tokens, wp), BF16),
        vm((parts, rows_w, wp), F32),
        vm((parts, a - 1, rows_w, wp), BF16),
        vm((parts, a - 1, rows_w, wp), BF16),
        vm((2, tokens, tw), F32),
        vm((dp - 1, 2, tokens, tw), F32),
        vm((2, tokens, tw), F32),
        vm((dp - 1, 2, tokens, tw), F32),
        vm((rows, width), F32),
        vm((a - 1, rows // a, width), F32),
        vm((b, rows // a, width), F32),
        vm((rows, width), F32),
        dma((2,)), dma((2,)),
        dma((b - 1,)), dma((b - 1,)),
        dma((b - 1, dp - 1)), dma((b - 1, dp - 1)),
        dma((parts, a - 1)), dma((parts, a - 1)),
        dma((dp - 1,)), dma((dp - 1,)), dma((dp - 1,)), dma((dp - 1,)),
        dma((parts, b - 1)), dma((parts, b - 1)),
        dma((parts, b - 1)), dma((parts, b - 1)),
        dma((parts, a - 1)), dma((parts, a - 1)),
        dma((a - 1,)), dma((a - 1,)),
        dma((b - 1,)), dma((b - 1,)),
        dma((a - 1,)), dma((a - 1,)),
    ]
    spec = pl.BlockSpec(memory_space=pltpu.VMEM)
    anywhere = pl.BlockSpec(memory_space=pl.ANY)
    results = pl.pallas_call(
        functools.partial(kernel, (a, b, dp)),
        out_shape=(
            jax.ShapeDtypeStruct((tokens, width), BF16),
            jax.ShapeDtypeStruct((tokens, width), BF16),
            jax.ShapeDtypeStruct((rows_w, width), F32),
            jax.ShapeDtypeStruct((rows, width), F32),
        ),
        in_specs=[anywhere] * 4 + [spec] * 2,
        out_specs=(spec,) * 4,
        scratch_shapes=scratch,
        compiler_params=pltpu.CompilerParams(
            collective_id=0, has_side_effects=True, vmem_limit_bytes=56 * 1024 * 1024),
    )(val, gate, cot, w, taps, gain)
    return pl.pallas_call(
        finish,
        out_shape=(
            jax.ShapeDtypeStruct((tokens, width), BF16),
            jax.ShapeDtypeStruct((tokens, width), BF16),
            jax.ShapeDtypeStruct((rows_w, width), F32),
            jax.ShapeDtypeStruct((taps_n, width), F32),
            jax.ShapeDtypeStruct((width,), F32),
        ),
        in_specs=[spec] * 4,
        out_specs=(spec,) * 5,
    )(*results)


def solution(mesh):
    in_specs = (P("sp", "dp"), P("sp", "dp"), P("sp", None), P("sp", "dp"), P(None, "dp"), P("dp"))
    out_specs = (P("sp", "dp"), P("sp", "dp"), P("sp", "dp"), P(None, "dp"), P("dp"))
    run = functools.partial(body, mesh.shape["sp"], mesh.shape["dp"])
    return jax.shard_map(run, mesh=mesh, in_specs=in_specs, out_specs=out_specs, check_vma=False)
```

```python
import functools

import jax
import jax.numpy as jnp
from jax import lax
from jax.experimental import pallas as pl
from jax.experimental.pallas import tpu as pltpu
from jax.sharding import PartitionSpec as P

norm_floor = 0.25
F32 = jnp.float32
BF16 = jnp.bfloat16
LOW = 4


def kernel(dims, val_in, gate_in, cot, w, taps, gain, gv, gg, gw, gt,
           val, gate, loads, cott, pin, gcp, nrm, dact, cbuf, sgm, acc1, acc2, inv,
           hs1, hr1, hs2, hr2, cotg, wg, swg, own_mix, mixs, mixr, own_gw, gws, gwr,
           ps1, pr1, ps2, pr2, red, r1, r2, gts,
           h1, h2, cs, cr, fs, fr, ws, wr, p1s, p1r, p2s, p2r, ss, sr, ms, mr, gs, gr,
           t1s, t1r, t2s, t2r, t3s, t3r):
    a, b, dp = dims
    sp = a * b
    tokens, width = val.shape
    taps_n = taps.shape[0]
    channels = width * dp
    chunks, halo_len, tw = pin.shape
    halo = halo_len - tokens
    base = halo - (taps_n - 1)
    rows_w = w.shape[0]
    depth = cotg.shape[1]
    parts, _, wp = wg.shape
    per = chunks // parts
    part_t = tokens // dp
    rows_r = red.shape[0] // a

    s = lax.axis_index("sp")
    c = lax.axis_index("dp")
    hi = s // a
    lo = lax.rem(s, a)

    def hi_peer(j):
        return (lax.rem(hi + j, b) * a + lo, c)

    def lo_peer(j):
        return (hi * a + lax.rem(lo + j, a), c)

    def dp_peer(j):
        return (s, lax.rem(c + j, dp))

    after = (lax.rem(s + 1, sp), c)
    before = (lax.rem(s + sp - 1, sp), c)

    def remote(src, dst, send, recv, to):
        return pltpu.make_async_remote_copy(
            src_ref=src, dst_ref=dst, send_sem=send, recv_sem=recv,
            device_id=to, device_id_type=pl.DeviceIdType.MESH)

    def lanes(i):
        if chunks == 1:
            return pl.ds(0, tw)
        return pl.ds(pl.multiple_of(i * tw, tw), tw)

    def place(i):
        if parts == 1:
            return 0, lanes(i)
        return i // per, pl.ds(pl.multiple_of(lax.rem(i, per) * tw, tw), tw)

    own_rows = pl.ds(pl.multiple_of(hi * tokens, tokens), tokens)
    own_depth = pl.ds(pl.multiple_of(lo * rows_w, rows_w), rows_w)
    barrier = pltpu.get_barrier_semaphore()
    peers = ([after, before] + [hi_peer(j) for j in range(1, b)]
             + [lo_peer(j) for j in range(1, a)] + [dp_peer(j) for j in range(1, dp)])
    for peer in peers:
        pl.semaphore_signal(barrier, inc=1, device_id=peer, device_id_type=pl.DeviceIdType.MESH)

    local = [pltpu.make_async_copy(val_in, val, loads.at[0]),
             pltpu.make_async_copy(gate_in, gate, loads.at[1]),
             pltpu.make_async_copy(cot.at[:, pl.ds(pl.multiple_of(hi * depth, 128), depth)],
                                   cotg.at[own_rows, :], loads.at[2])]
    for h in range(parts):
        local.append(pltpu.make_async_copy(w.at[:, h * wp:(h + 1) * wp], wg.at[h, own_depth, :], loads.at[3 + h]))
    for copy in local:
        copy.start()
    local[0].wait()
    local[1].wait()

    @pl.loop(0, chunks)
    def _(i):
        at = lanes(i)
        sig = jax.nn.sigmoid(gate[:, at].astype(F32))
        sgm[i] = sig
        mixed = (val[:, at].astype(F32) * sig).astype(BF16)
        hs1[:, at] = mixed[tokens - halo:]
        pin[i, halo:, :] = mixed.astype(F32)

    pl.semaphore_wait(barrier, len(peers))

    sends = []
    halo1 = remote(hs1, hr1, h1.at[0], h1.at[1], after)
    halo1.start()
    my_rows = pl.ds(pl.multiple_of(c * part_t, part_t), part_t)
    cot_in = []
    for j in range(1, b):
        other = lax.rem(hi + j, b)
        copy = remote(cot.at[my_rows, pl.ds(pl.multiple_of(other * depth, 128), depth)],
                      cotg.at[pl.ds(pl.multiple_of(hi * tokens + c * part_t, part_t), part_t), :],
                      cs.at[j - 1], cr.at[j - 1], hi_peer(j))
        copy.start()
        cot_in.append(copy)
    w_in = [[] for _ in range(parts)]
    for h in range(parts):
        for j in range(1, a):
            copy = remote(w.at[:, h * wp:(h + 1) * wp], wg.at[h, own_depth, :],
                          ws.at[h, j - 1], wr.at[h, j - 1], lo_peer(j))
            copy.start()
            w_in[h].append(copy)
    sends += [halo1] + cot_in + sum(w_in, [])

    halo1.wait_recv()
    keep_first = (s > 0).astype(F32)
    acc1[...] = jnp.zeros_like(acc1)
    acc2[...] = jnp.zeros_like(acc2)

    @pl.loop(0, chunks)
    def _(i):
        at = lanes(i)
        pin[i, :halo, :] = hr1[:, at].astype(F32) * keep_first
        total = jnp.zeros((tokens, tw), F32)
        for k in range(taps_n):
            total = total + taps[k:k + 1, at] * pin[i, base + k:base + k + tokens, :]
        rounded = total.astype(BF16).astype(F32)
        cbuf[i] = rounded
        acc1[...] += rounded
        acc2[...] += rounded * rounded

    def share(buf, got, send, recv):
        buf[0] = jnp.broadcast_to(jnp.sum(acc1[...], 1, keepdims=True), (tokens, tw))
        buf[1] = jnp.broadcast_to(jnp.sum(acc2[...], 1, keepdims=True), (tokens, tw))
        copies = []
        for j in range(1, dp):
            copy = remote(buf, got.at[j - 1], send.at[j - 1], recv.at[j - 1], dp_peer(j))
            copy.start()
            copies.append(copy)
        return copies

    def gathered(buf, got, copies):
        for copy in copies:
            copy.wait_recv()
        for j in range(1, dp):
            buf_sum = got[j - 1]
            acc1[...] = (buf[0] if j == 1 else acc1[...]) + buf_sum[0]
            acc2[...] = (buf[1] if j == 1 else acc2[...]) + buf_sum[1]

    first = share(ps1, pr1, p1s, p1r)
    gathered(ps1, pr1, first)
    sends += first
    mean = acc1[...] / channels
    inv[...] = lax.rsqrt(acc2[...] / channels - mean * mean + norm_floor)
    acc1[...] = mean

    @pl.loop(0, chunks)
    def _(i):
        at = lanes(i)
        normed = (cbuf[i] - acc1[...]) * inv[...]
        act = normed * gain[at][None, :]
        part, within = place(i)
        sig = jax.nn.sigmoid(act)
        swg[part, own_rows, within] = (act * sig).astype(BF16)
        nrm[i] = normed
        dact[i] = sig * (1.0 + act * (1.0 - sig))

    def sw_copy(step, up, source):
        rows = swg.at[:, pl.ds(pl.multiple_of(source * tokens, tokens), tokens), :]
        way = 0 if up else 1
        return remote(rows, rows, ss.at[way, step], sr.at[way, step], hi_peer(1 if up else b - 1))

    def sw_send(step, finish_it=False):
        for up in (True, False):
            source = hi - step if up else hi + step
            here = (source >= 0) & (hi + 1 < b) if up else (source < b) & (hi > 0)

            @pl.when(here)
            def _():
                copy = sw_copy(step, up, source)
                if finish_it:
                    copy.wait_send()
                else:
                    copy.start()

    def sw_take(step):
        for up in (True, False):
            source = hi - 1 - step if up else hi + 1 + step

            @pl.when(source >= 0 if up else source < b)
            def _():
                sw_copy(step, up, source).wait_recv()

    sw_send(0)

    forwards = []
    for j in range(1, b):
        cot_in[j - 1].wait_recv()
        origin = lax.rem(hi + b - j, b)
        rows = cotg.at[pl.ds(pl.multiple_of(origin * tokens + c * part_t, part_t), part_t), :]
        for d in range(1, dp):
            copy = remote(rows, rows, fs.at[j - 1, d - 1], fr.at[j - 1, d - 1], dp_peer(d))
            copy.start()
            forwards.append(copy)
    sends += forwards
    for copy in local[2:]:
        copy.wait()
    for copy in forwards:
        copy.wait_recv()

    def mix_copy(h, j):
        return remote(mixs.at[h, j - 1], mixr.at[h, j - 1], ms.at[h, j - 1], mr.at[h, j - 1], hi_peer(j))

    step = 0
    for h in range(parts):
        if step < b - 2:
            sw_take(step)
            step += 1
            sw_send(step)
        for copy in w_in[h]:
            copy.wait_recv()

        @pl.loop(1, b)
        def _(j):
            other = lax.rem(hi + j, b)
            block = cotg[pl.ds(pl.multiple_of(other * tokens, tokens), tokens), :]
            mixs[h, j - 1] = jnp.dot(block, wg[h], preferred_element_type=F32).astype(BF16)
            mix_copy(h, j).start()

    for h in range(parts):
        own_mix[h] = jnp.dot(cotg[own_rows, :], wg[h], preferred_element_type=F32)
    for q in range(a):
        cott[q * rows_w:(q + 1) * rows_w, :] = cotg[:, q * rows_w:(q + 1) * rows_w].T

    def gw_copy(h, j):
        return remote(gws.at[h, j - 1], gwr.at[h, j - 1], gs.at[h, j - 1], gr.at[h, j - 1], lo_peer(j))

    def gw_part(h):
        @pl.loop(1, a)
        def _(j):
            other = lax.rem(lo + j, a)
            block = cott[pl.ds(pl.multiple_of(other * rows_w, rows_w), rows_w), :]
            gws[h, j - 1] = jnp.dot(block, swg[h], preferred_element_type=F32).astype(BF16)
            gw_copy(h, j).start()

        own_gw[h] = jnp.dot(cott[own_depth, :], swg[h], preferred_element_type=F32)

    while step < b - 2:
        sw_take(step)
        step += 1
        sw_send(step)
    if b > 1:
        sw_take(b - 2)
    for h in range(parts):
        gw_part(h)

    for h in range(parts):
        for j in range(1, b):
            mix_copy(h, j).wait_recv()
    acc1[...] = jnp.zeros_like(acc1)
    acc2[...] = jnp.zeros_like(acc2)
    red[...] = jnp.zeros_like(red)

    @pl.loop(0, chunks)
    def _(i):
        at = lanes(i)
        part, within = place(i)
        mix = own_mix[part, :, within]
        for j in range(1, b):
            mix = mix + mixr[part, j - 1, :, within].astype(F32)
        grad_act = mix * dact[i]
        normed = nrm[i]
        red[taps_n:taps_n + 1, at] = jnp.sum(grad_act * normed, 0, keepdims=True)
        grad_norm = grad_act * gain[at][None, :]
        cbuf[i] = grad_norm
        acc1[...] += grad_norm
        acc2[...] += grad_norm * normed

    second = share(ps2, pr2, p2s, p2r)
    gathered(ps2, pr2, second)
    sends += second
    acc1[...] = acc1[...] / channels
    acc2[...] = acc2[...] / channels

    @pl.loop(0, chunks)
    def _(i):
        at = lanes(i)
        rounded = (inv[...] * (cbuf[i] - acc1[...] - nrm[i] * acc2[...])).astype(BF16)
        hs2[:, at] = rounded[:halo]
        gcp[i, :tokens, :] = rounded.astype(F32)

    halo2 = remote(hs2, hr2, h2.at[0], h2.at[1], before)
    halo2.start()
    sends.append(halo2)

    @pl.loop(0, chunks)
    def _(i):
        at = lanes(i)
        grad = gcp[i, :tokens, :]
        for k in range(taps_n):
            red[k:k + 1, at] = jnp.sum(grad * pin[i, base + k:base + k + tokens, :], 0, keepdims=True)

    stage1 = []
    for j in range(1, a):
        other = lax.rem(lo + j, a)
        copy = remote(red.at[pl.ds(pl.multiple_of(other * rows_r, 8), rows_r), :], r1.at[j - 1],
                      t1s.at[j - 1], t1r.at[j - 1], lo_peer(j))
        copy.start()
        stage1.append(copy)
    sends += stage1

    halo2.wait_recv()
    keep_last = (s < sp - 1).astype(F32)

    @pl.loop(0, chunks)
    def _(i):
        at = lanes(i)
        gcp[i, tokens:, :] = hr2[:, at].astype(F32) * keep_last
        total = jnp.zeros((tokens, tw), F32)
        for k in range(taps_n):
            back = taps_n - 1 - k
            total = total + taps[k:k + 1, at] * gcp[i, back:back + tokens, :]
        grad = total.astype(BF16).astype(F32)
        sig = sgm[i]
        gv[:, at] = (grad * sig).astype(BF16)
        gg[:, at] = (grad * val[:, at].astype(F32) * sig * (1.0 - sig)).astype(BF16)

    for copy in stage1:
        copy.wait_recv()
    mine = red[pl.ds(pl.multiple_of(lo * rows_r, 8), rows_r), :]
    for j in range(1, a):
        mine = mine + r1[j - 1]
    r2[hi] = mine
    stage2 = []
    for j in range(1, b):
        copy = remote(r2.at[hi], r2.at[hi], t2s.at[j - 1], t2r.at[j - 1], hi_peer(j))
        copy.start()
        stage2.append(copy)
    sends += stage2
    for copy in stage2:
        copy.wait_recv()
    summed = r2[0]
    for j in range(1, b):
        summed = summed + r2[j]
    my_red = pl.ds(pl.multiple_of(lo * rows_r, 8), rows_r)
    gts[my_red, :] = summed
    stage3 = []
    for j in range(1, a):
        copy = remote(gts.at[my_red, :], gts.at[my_red, :], t3s.at[j - 1], t3r.at[j - 1], lo_peer(j))
        copy.start()
        stage3.append(copy)
    sends += stage3

    for h in range(parts):
        for j in range(1, a):
            gw_copy(h, j).wait_recv()
        total = own_gw[h]
        for j in range(1, a):
            total = total + gwr[h, j - 1].astype(F32)
        gw[:, h * wp:(h + 1) * wp] = total

    for copy in stage3:
        copy.wait_recv()
    gt[...] = gts[...]

    for copy in sends:
        copy.wait_send()
    for step in range(b - 1):
        sw_send(step, True)
    for h in range(parts):
        for j in range(1, b):
            mix_copy(h, j).wait_send()
        for j in range(1, a):
            gw_copy(h, j).wait_send()


def finish(gv, gg, gw, gt, out_gv, out_gg, out_gw, out_taps, out_gain):
    out_gv[...] = gv[...]
    out_gg[...] = gg[...]
    out_gw[...] = gw[...]
    taps_n = out_taps.shape[0]
    out_taps[...] = gt[:taps_n]
    out_gain[...] = gt[taps_n]


def body(sp, dp, val, gate, cot, w, taps, gain):
    a = LOW if sp % LOW == 0 else 1
    b = sp // a
    tokens, width = val.shape
    rows_w = w.shape[0]
    model = cot.shape[1]
    depth = model // b
    taps_n = taps.shape[0]
    tw = 128 if width % 128 == 0 else width
    chunks = width // tw
    halo = -(-(taps_n - 1) // 16) * 16
    rows = -(-(taps_n + 1) // (8 * a)) * 8 * a
    parts = 3 if chunks % 3 == 0 else 2 if chunks % 2 == 0 else 1
    wp = width // parts
    vm, dma = pltpu.VMEM, pltpu.SemaphoreType.DMA
    scratch = [
        vm((tokens, width), BF16),
        vm((tokens, width), BF16),
        dma((3 + parts,)),
        vm((depth, b * tokens), BF16),
        vm((chunks, tokens + halo, tw), F32),
        vm((chunks, tokens + halo, tw), F32),
        vm((chunks, tokens, tw), F32),
        vm((chunks, tokens, tw), F32),
        vm((chunks, tokens, tw), F32),
        vm((chunks, tokens, tw), F32),
        vm((tokens, tw), F32),
        vm((tokens, tw), F32),
        vm((tokens, tw), F32),
        vm((halo, width), BF16),
        vm((halo, width), BF16),
        vm((halo, width), BF16),
        vm((halo, width), BF16),
        vm((b * tokens, depth), BF16),
        vm((parts, depth, wp), BF16),
        vm((parts, b * tokens, wp), BF16),
        vm((parts, tokens, wp), F32),
        vm((parts, b - 1, tokens, wp), BF16),
        vm((parts, b - 1, tokens, wp), BF16),
        vm((parts, rows_w, wp), F32),
        vm((parts, a - 1, rows_w, wp), BF16),
        vm((parts, a - 1, rows_w, wp), BF16),
        vm((2, tokens, tw), F32),
        vm((dp - 1, 2, tokens, tw), F32),
        vm((2, tokens, tw), F32),
        vm((dp - 1, 2, tokens, tw), F32),
        vm((rows, width), F32),
        vm((a - 1, rows // a, width), F32),
        vm((b, rows // a, width), F32),
        vm((rows, width), F32),
        dma((2,)), dma((2,)),
        dma((b - 1,)), dma((b - 1,)),
        dma((b - 1, dp - 1)), dma((b - 1, dp - 1)),
        dma((parts, a - 1)), dma((parts, a - 1)),
        dma((dp - 1,)), dma((dp - 1,)), dma((dp - 1,)), dma((dp - 1,)),
        dma((2, b - 1)), dma((2, b - 1)),
        dma((parts, b - 1)), dma((parts, b - 1)),
        dma((parts, a - 1)), dma((parts, a - 1)),
        dma((a - 1,)), dma((a - 1,)),
        dma((b - 1,)), dma((b - 1,)),
        dma((a - 1,)), dma((a - 1,)),
    ]
    spec = pl.BlockSpec(memory_space=pltpu.VMEM)
    anywhere = pl.BlockSpec(memory_space=pl.ANY)
    results = pl.pallas_call(
        functools.partial(kernel, (a, b, dp)),
        out_shape=(
            jax.ShapeDtypeStruct((tokens, width), BF16),
            jax.ShapeDtypeStruct((tokens, width), BF16),
            jax.ShapeDtypeStruct((rows_w, width), F32),
            jax.ShapeDtypeStruct((rows, width), F32),
        ),
        in_specs=[anywhere] * 4 + [spec] * 2,
        out_specs=(spec,) * 4,
        scratch_shapes=scratch,
        compiler_params=pltpu.CompilerParams(
            collective_id=0, has_side_effects=True, vmem_limit_bytes=56 * 1024 * 1024),
    )(val, gate, cot, w, taps, gain)
    return pl.pallas_call(
        finish,
        out_shape=(
            jax.ShapeDtypeStruct((tokens, width), BF16),
            jax.ShapeDtypeStruct((tokens, width), BF16),
            jax.ShapeDtypeStruct((rows_w, width), F32),
            jax.ShapeDtypeStruct((taps_n, width), F32),
            jax.ShapeDtypeStruct((width,), F32),
        ),
        in_specs=[spec] * 4,
        out_specs=(spec,) * 5,
    )(*results)


def solution(mesh):
    in_specs = (P("sp", "dp"), P("sp", "dp"), P("sp", None), P("sp", "dp"), P(None, "dp"), P("dp"))
    out_specs = (P("sp", "dp"), P("sp", "dp"), P("sp", "dp"), P(None, "dp"), P("dp"))
    run = functools.partial(body, mesh.shape["sp"], mesh.shape["dp"])
    return jax.shard_map(run, mesh=mesh, in_specs=in_specs, out_specs=out_specs, check_vma=False)
```

```python
import functools

import jax
import jax.numpy as jnp
from jax import lax
from jax.experimental import pallas as pl
from jax.experimental.pallas import tpu as pltpu
from jax.sharding import PartitionSpec as P

norm_floor = 0.25
F32 = jnp.float32
BF16 = jnp.bfloat16
LOW = 4


def kernel(dims, val_in, gate_in, cot, w, taps, gain, gv, gg, gw, gt,
           val, gate, loads, cott, pin, gcp, nrm, dact, cbuf, sgm, acc1, acc2, inv,
           hs1, hr1, hs2, hr2, cotg, wg, swg, own_mix, mixs, mixr, own_gw, gws, gwr,
           ps1, pr1, ps2, pr2, red, r1, r2, gts,
           h1, h2, cs, cr, fs, fr, ws, wr, p1s, p1r, p2s, p2r, ss, sr, ms, mr, gs, gr,
           t1s, t1r, t2s, t2r, t3s, t3r):
    a, b, dp = dims
    sp = a * b
    tokens, width = val.shape
    taps_n = taps.shape[0]
    channels = width * dp
    chunks, halo_len, tw = pin.shape
    halo = halo_len - tokens
    base = halo - (taps_n - 1)
    rows_w = w.shape[0]
    depth = cotg.shape[1]
    parts, _, wp = wg.shape
    per = chunks // parts
    part_t = tokens // dp
    rows_r = red.shape[0] // a

    s = lax.axis_index("sp")
    c = lax.axis_index("dp")
    hi = s // a
    lo = lax.rem(s, a)

    def hi_peer(j):
        return (lax.rem(hi + j, b) * a + lo, c)

    def lo_peer(j):
        return (hi * a + lax.rem(lo + j, a), c)

    def dp_peer(j):
        return (s, lax.rem(c + j, dp))

    after = (lax.rem(s + 1, sp), c)
    before = (lax.rem(s + sp - 1, sp), c)

    def remote(src, dst, send, recv, to):
        return pltpu.make_async_remote_copy(
            src_ref=src, dst_ref=dst, send_sem=send, recv_sem=recv,
            device_id=to, device_id_type=pl.DeviceIdType.MESH)

    def lanes(i):
        if chunks == 1:
            return pl.ds(0, tw)
        return pl.ds(pl.multiple_of(i * tw, tw), tw)

    def place(i):
        if parts == 1:
            return 0, lanes(i)
        return i // per, pl.ds(pl.multiple_of(lax.rem(i, per) * tw, tw), tw)

    own_rows = pl.ds(pl.multiple_of(hi * tokens, tokens), tokens)
    own_depth = pl.ds(pl.multiple_of(lo * rows_w, rows_w), rows_w)
    barrier = pltpu.get_barrier_semaphore()
    peers = ([after, before] + [hi_peer(j) for j in range(1, b)]
             + [lo_peer(j) for j in range(1, a)] + [dp_peer(j) for j in range(1, dp)])
    for peer in peers:
        pl.semaphore_signal(barrier, inc=1, device_id=peer, device_id_type=pl.DeviceIdType.MESH)

    local = [pltpu.make_async_copy(val_in, val, loads.at[0]),
             pltpu.make_async_copy(gate_in, gate, loads.at[1]),
             pltpu.make_async_copy(cot.at[:, pl.ds(pl.multiple_of(hi * depth, 128), depth)],
                                   cotg.at[own_rows, :], loads.at[2])]
    for h in range(parts):
        local.append(pltpu.make_async_copy(w.at[:, h * wp:(h + 1) * wp], wg.at[h, own_depth, :], loads.at[3 + h]))
    for copy in local:
        copy.start()
    local[0].wait()
    local[1].wait()

    @pl.loop(0, chunks)
    def _(i):
        at = lanes(i)
        sig = jax.nn.sigmoid(gate[:, at].astype(F32))
        sgm[i] = sig
        mixed = (val[:, at].astype(F32) * sig).astype(BF16)
        hs1[:, at] = mixed[tokens - halo:]
        pin[i, halo:, :] = mixed.astype(F32)

    pl.semaphore_wait(barrier, len(peers))

    sends = []
    halo1 = remote(hs1, hr1, h1.at[0], h1.at[1], after)
    halo1.start()
    my_rows = pl.ds(pl.multiple_of(c * part_t, part_t), part_t)
    cot_in = []
    for j in range(1, b):
        other = lax.rem(hi + j, b)
        copy = remote(cot.at[my_rows, pl.ds(pl.multiple_of(other * depth, 128), depth)],
                      cotg.at[pl.ds(pl.multiple_of(hi * tokens + c * part_t, part_t), part_t), :],
                      cs.at[j - 1], cr.at[j - 1], hi_peer(j))
        copy.start()
        cot_in.append(copy)
    w_in = [[] for _ in range(parts)]
    for h in range(parts):
        for j in range(1, a):
            copy = remote(w.at[:, h * wp:(h + 1) * wp], wg.at[h, own_depth, :],
                          ws.at[h, j - 1], wr.at[h, j - 1], lo_peer(j))
            copy.start()
            w_in[h].append(copy)
    sends += [halo1] + cot_in + sum(w_in, [])

    halo1.wait_recv()
    keep_first = (s > 0).astype(F32)
    acc1[...] = jnp.zeros_like(acc1)
    acc2[...] = jnp.zeros_like(acc2)

    @pl.loop(0, chunks)
    def _(i):
        at = lanes(i)
        pin[i, :halo, :] = hr1[:, at].astype(F32) * keep_first
        total = jnp.zeros((tokens, tw), F32)
        for k in range(taps_n):
            total = total + taps[k:k + 1, at] * pin[i, base + k:base + k + tokens, :]
        rounded = total.astype(BF16).astype(F32)
        cbuf[i] = rounded
        acc1[...] += rounded
        acc2[...] += rounded * rounded

    def share(buf, got, send, recv):
        buf[0] = jnp.broadcast_to(jnp.sum(acc1[...], 1, keepdims=True), (tokens, tw))
        buf[1] = jnp.broadcast_to(jnp.sum(acc2[...], 1, keepdims=True), (tokens, tw))
        copies = []
        for j in range(1, dp):
            copy = remote(buf, got.at[j - 1], send.at[j - 1], recv.at[j - 1], dp_peer(j))
            copy.start()
            copies.append(copy)
        return copies

    def gathered(buf, got, copies):
        for copy in copies:
            copy.wait_recv()
        for j in range(1, dp):
            buf_sum = got[j - 1]
            acc1[...] = (buf[0] if j == 1 else acc1[...]) + buf_sum[0]
            acc2[...] = (buf[1] if j == 1 else acc2[...]) + buf_sum[1]

    first = share(ps1, pr1, p1s, p1r)
    gathered(ps1, pr1, first)
    sends += first
    mean = acc1[...] / channels
    inv[...] = lax.rsqrt(acc2[...] / channels - mean * mean + norm_floor)
    acc1[...] = mean

    @pl.loop(0, chunks)
    def _(i):
        at = lanes(i)
        normed = (cbuf[i] - acc1[...]) * inv[...]
        act = normed * gain[at][None, :]
        part, within = place(i)
        sig = jax.nn.sigmoid(act)
        swg[part, own_rows, within] = (act * sig).astype(BF16)
        nrm[i] = normed
        dact[i] = sig * (1.0 + act * (1.0 - sig))

    def sw_copy(step, up, source):
        rows = swg.at[:, pl.ds(pl.multiple_of(source * tokens, tokens), tokens), :]
        way = 0 if up else 1
        return remote(rows, rows, ss.at[way, step], sr.at[way, step], hi_peer(1 if up else b - 1))

    def sw_send(step, finish_it=False):
        for up in (True, False):
            source = hi - step if up else hi + step
            here = (source >= 0) & (hi + 1 < b) if up else (source < b) & (hi > 0)

            @pl.when(here)
            def _():
                copy = sw_copy(step, up, source)
                if finish_it:
                    copy.wait_send()
                else:
                    copy.start()

    def sw_take(step):
        for up in (True, False):
            source = hi - 1 - step if up else hi + 1 + step

            @pl.when(source >= 0 if up else source < b)
            def _():
                sw_copy(step, up, source).wait_recv()

    sw_send(0)

    forwards = []
    for j in range(1, b):
        cot_in[j - 1].wait_recv()
        origin = lax.rem(hi + b - j, b)
        rows = cotg.at[pl.ds(pl.multiple_of(origin * tokens + c * part_t, part_t), part_t), :]
        for d in range(1, dp):
            copy = remote(rows, rows, fs.at[j - 1, d - 1], fr.at[j - 1, d - 1], dp_peer(d))
            copy.start()
            forwards.append(copy)
    sends += forwards
    for copy in local[2:]:
        copy.wait()
    for copy in forwards:
        copy.wait_recv()

    def mix_copy(h, j):
        return remote(mixs.at[h, j - 1], mixr.at[h, j - 1], ms.at[h, j - 1], mr.at[h, j - 1], hi_peer(j))

    for step in range(b - 2):
        sw_take(step)
        sw_send(step + 1)
    for h in range(parts):
        for copy in w_in[h]:
            copy.wait_recv()

        @pl.loop(1, b)
        def _(j):
            other = lax.rem(hi + j, b)
            block = cotg[pl.ds(pl.multiple_of(other * tokens, tokens), tokens), :]
            mixs[h, j - 1] = jnp.dot(block, wg[h], preferred_element_type=F32).astype(BF16)
            mix_copy(h, j).start()

    for h in range(parts):
        own_mix[h] = jnp.dot(cotg[own_rows, :], wg[h], preferred_element_type=F32)
    for q in range(a):
        cott[q * rows_w:(q + 1) * rows_w, :] = cotg[:, q * rows_w:(q + 1) * rows_w].T

    def gw_copy(h, j):
        return remote(gws.at[h, j - 1], gwr.at[h, j - 1], gs.at[h, j - 1], gr.at[h, j - 1], lo_peer(j))

    def gw_part(h):
        @pl.loop(1, a)
        def _(j):
            other = lax.rem(lo + j, a)
            block = cott[pl.ds(pl.multiple_of(other * rows_w, rows_w), rows_w), :]
            gws[h, j - 1] = jnp.dot(block, swg[h], preferred_element_type=F32).astype(BF16)
            gw_copy(h, j).start()

        own_gw[h] = jnp.dot(cott[own_depth, :], swg[h], preferred_element_type=F32)

    if b > 1:
        sw_take(b - 2)
    for h in range(max(parts - 1, 1)):
        gw_part(h)

    for h in range(parts):
        for j in range(1, b):
            mix_copy(h, j).wait_recv()
    acc1[...] = jnp.zeros_like(acc1)
    acc2[...] = jnp.zeros_like(acc2)
    red[...] = jnp.zeros_like(red)

    @pl.loop(0, chunks)
    def _(i):
        at = lanes(i)
        part, within = place(i)
        mix = own_mix[part, :, within]
        for j in range(1, b):
            mix = mix + mixr[part, j - 1, :, within].astype(F32)
        grad_act = mix * dact[i]
        normed = nrm[i]
        red[taps_n:taps_n + 1, at] = jnp.sum(grad_act * normed, 0, keepdims=True)
        grad_norm = grad_act * gain[at][None, :]
        cbuf[i] = grad_norm
        acc1[...] += grad_norm
        acc2[...] += grad_norm * normed

    second = share(ps2, pr2, p2s, p2r)
    gathered(ps2, pr2, second)
    sends += second
    acc1[...] = acc1[...] / channels
    acc2[...] = acc2[...] / channels

    @pl.loop(0, chunks)
    def _(i):
        at = lanes(i)
        rounded = (inv[...] * (cbuf[i] - acc1[...] - nrm[i] * acc2[...])).astype(BF16)
        hs2[:, at] = rounded[:halo]
        gcp[i, :tokens, :] = rounded.astype(F32)

    halo2 = remote(hs2, hr2, h2.at[0], h2.at[1], before)
    halo2.start()
    sends.append(halo2)

    @pl.loop(0, chunks)
    def _(i):
        at = lanes(i)
        grad = gcp[i, :tokens, :]
        for k in range(taps_n):
            red[k:k + 1, at] = jnp.sum(grad * pin[i, base + k:base + k + tokens, :], 0, keepdims=True)

    stage1 = []
    for j in range(1, a):
        other = lax.rem(lo + j, a)
        copy = remote(red.at[pl.ds(pl.multiple_of(other * rows_r, 8), rows_r), :], r1.at[j - 1],
                      t1s.at[j - 1], t1r.at[j - 1], lo_peer(j))
        copy.start()
        stage1.append(copy)
    sends += stage1
    if parts > 1:
        gw_part(parts - 1)

    halo2.wait_recv()
    keep_last = (s < sp - 1).astype(F32)

    @pl.loop(0, chunks)
    def _(i):
        at = lanes(i)
        gcp[i, tokens:, :] = hr2[:, at].astype(F32) * keep_last
        total = jnp.zeros((tokens, tw), F32)
        for k in range(taps_n):
            back = taps_n - 1 - k
            total = total + taps[k:k + 1, at] * gcp[i, back:back + tokens, :]
        grad = total.astype(BF16).astype(F32)
        sig = sgm[i]
        gv[:, at] = (grad * sig).astype(BF16)
        gg[:, at] = (grad * val[:, at].astype(F32) * sig * (1.0 - sig)).astype(BF16)

    for copy in stage1:
        copy.wait_recv()
    mine = red[pl.ds(pl.multiple_of(lo * rows_r, 8), rows_r), :]
    for j in range(1, a):
        mine = mine + r1[j - 1]
    r2[hi] = mine
    stage2 = []
    for j in range(1, b):
        copy = remote(r2.at[hi], r2.at[hi], t2s.at[j - 1], t2r.at[j - 1], hi_peer(j))
        copy.start()
        stage2.append(copy)
    sends += stage2
    for copy in stage2:
        copy.wait_recv()
    summed = r2[0]
    for j in range(1, b):
        summed = summed + r2[j]
    my_red = pl.ds(pl.multiple_of(lo * rows_r, 8), rows_r)
    gts[my_red, :] = summed
    stage3 = []
    for j in range(1, a):
        copy = remote(gts.at[my_red, :], gts.at[my_red, :], t3s.at[j - 1], t3r.at[j - 1], lo_peer(j))
        copy.start()
        stage3.append(copy)
    sends += stage3

    for h in range(parts):
        for j in range(1, a):
            gw_copy(h, j).wait_recv()
        total = own_gw[h]
        for j in range(1, a):
            total = total + gwr[h, j - 1].astype(F32)
        gw[:, h * wp:(h + 1) * wp] = total

    for copy in stage3:
        copy.wait_recv()
    gt[...] = gts[...]

    for copy in sends:
        copy.wait_send()
    for step in range(b - 1):
        sw_send(step, True)
    for h in range(parts):
        for j in range(1, b):
            mix_copy(h, j).wait_send()
        for j in range(1, a):
            gw_copy(h, j).wait_send()


def finish(gv, gg, gw, gt, out_gv, out_gg, out_gw, out_taps, out_gain):
    out_gv[...] = gv[...]
    out_gg[...] = gg[...]
    out_gw[...] = gw[...]
    taps_n = out_taps.shape[0]
    out_taps[...] = gt[:taps_n]
    out_gain[...] = gt[taps_n]


def body(sp, dp, val, gate, cot, w, taps, gain):
    a = LOW if sp % LOW == 0 else 1
    b = sp // a
    tokens, width = val.shape
    rows_w = w.shape[0]
    model = cot.shape[1]
    depth = model // b
    taps_n = taps.shape[0]
    tw = 128 if width % 128 == 0 else width
    chunks = width // tw
    halo = -(-(taps_n - 1) // 16) * 16
    rows = -(-(taps_n + 1) // (8 * a)) * 8 * a
    parts = 3 if chunks % 3 == 0 else 2 if chunks % 2 == 0 else 1
    wp = width // parts
    vm, dma = pltpu.VMEM, pltpu.SemaphoreType.DMA
    scratch = [
        vm((tokens, width), BF16),
        vm((tokens, width), BF16),
        dma((3 + parts,)),
        vm((depth, b * tokens), BF16),
        vm((chunks, tokens + halo, tw), F32),
        vm((chunks, tokens + halo, tw), F32),
        vm((chunks, tokens, tw), F32),
        vm((chunks, tokens, tw), F32),
        vm((chunks, tokens, tw), F32),
        vm((chunks, tokens, tw), F32),
        vm((tokens, tw), F32),
        vm((tokens, tw), F32),
        vm((tokens, tw), F32),
        vm((halo, width), BF16),
        vm((halo, width), BF16),
        vm((halo, width), BF16),
        vm((halo, width), BF16),
        vm((b * tokens, depth), BF16),
        vm((parts, depth, wp), BF16),
        vm((parts, b * tokens, wp), BF16),
        vm((parts, tokens, wp), F32),
        vm((parts, b - 1, tokens, wp), BF16),
        vm((parts, b - 1, tokens, wp), BF16),
        vm((parts, rows_w, wp), F32),
        vm((parts, a - 1, rows_w, wp), BF16),
        vm((parts, a - 1, rows_w, wp), BF16),
        vm((2, tokens, tw), F32),
        vm((dp - 1, 2, tokens, tw), F32),
        vm((2, tokens, tw), F32),
        vm((dp - 1, 2, tokens, tw), F32),
        vm((rows, width), F32),
        vm((a - 1, rows // a, width), F32),
        vm((b, rows // a, width), F32),
        vm((rows, width), F32),
        dma((2,)), dma((2,)),
        dma((b - 1,)), dma((b - 1,)),
        dma((b - 1, dp - 1)), dma((b - 1, dp - 1)),
        dma((parts, a - 1)), dma((parts, a - 1)),
        dma((dp - 1,)), dma((dp - 1,)), dma((dp - 1,)), dma((dp - 1,)),
        dma((2, b - 1)), dma((2, b - 1)),
        dma((parts, b - 1)), dma((parts, b - 1)),
        dma((parts, a - 1)), dma((parts, a - 1)),
        dma((a - 1,)), dma((a - 1,)),
        dma((b - 1,)), dma((b - 1,)),
        dma((a - 1,)), dma((a - 1,)),
    ]
    spec = pl.BlockSpec(memory_space=pltpu.VMEM)
    anywhere = pl.BlockSpec(memory_space=pl.ANY)
    results = pl.pallas_call(
        functools.partial(kernel, (a, b, dp)),
        out_shape=(
            jax.ShapeDtypeStruct((tokens, width), BF16),
            jax.ShapeDtypeStruct((tokens, width), BF16),
            jax.ShapeDtypeStruct((rows_w, width), F32),
            jax.ShapeDtypeStruct((rows, width), F32),
        ),
        in_specs=[anywhere] * 4 + [spec] * 2,
        out_specs=(spec,) * 4,
        scratch_shapes=scratch,
        compiler_params=pltpu.CompilerParams(
            collective_id=0, has_side_effects=True, vmem_limit_bytes=56 * 1024 * 1024),
    )(val, gate, cot, w, taps, gain)
    return pl.pallas_call(
        finish,
        out_shape=(
            jax.ShapeDtypeStruct((tokens, width), BF16),
            jax.ShapeDtypeStruct((tokens, width), BF16),
            jax.ShapeDtypeStruct((rows_w, width), F32),
            jax.ShapeDtypeStruct((taps_n, width), F32),
            jax.ShapeDtypeStruct((width,), F32),
        ),
        in_specs=[spec] * 4,
        out_specs=(spec,) * 5,
    )(*results)


def solution(mesh):
    in_specs = (P("sp", "dp"), P("sp", "dp"), P("sp", None), P("sp", "dp"), P(None, "dp"), P("dp"))
    out_specs = (P("sp", "dp"), P("sp", "dp"), P("sp", "dp"), P(None, "dp"), P("dp"))
    run = functools.partial(body, mesh.shape["sp"], mesh.shape["dp"])
    return jax.shard_map(run, mesh=mesh, in_specs=in_specs, out_specs=out_specs, check_vma=False)
```

```python
import functools

import jax
import jax.numpy as jnp
from jax import lax
from jax.experimental import pallas as pl
from jax.experimental.pallas import tpu as pltpu
from jax.sharding import PartitionSpec as P

norm_floor = 0.25
F32 = jnp.float32
BF16 = jnp.bfloat16
LOW = 4


def kernel(dims, val_in, gate_in, cot, w, taps, gain, gv, gg, gw, gt,
           val, gate, loads, cott, pin, gcp, nrm, dact, cbuf, sgm, acc1, acc2, inv,
           hs1, hr1, hs2, hr2, cotg, wg, swg, own_mix, mixs, mixr, own_gw, gws, gwr,
           ps1, pr1, ps2, pr2, red, r1, r2, gts,
           h1, h2, cs, cr, fs, fr, ws, wr, p1s, p1r, p2s, p2r, ss, sr, ms, mr, gs, gr,
           t1s, t1r, t2s, t2r, t3s, t3r):
    a, b, dp = dims
    sp = a * b
    tokens, width = val.shape
    taps_n = taps.shape[0]
    channels = width * dp
    chunks, halo_len, tw = pin.shape
    halo = halo_len - tokens
    base = halo - (taps_n - 1)
    rows_w = w.shape[0]
    depth = cotg.shape[1]
    parts, _, wp = wg.shape
    per = chunks // parts
    part_t = tokens // dp
    rows_r = red.shape[0] // a

    s = lax.axis_index("sp")
    c = lax.axis_index("dp")
    hi = s // a
    lo = lax.rem(s, a)

    def hi_peer(j):
        return (lax.rem(hi + j, b) * a + lo, c)

    def lo_peer(j):
        return (hi * a + lax.rem(lo + j, a), c)

    def dp_peer(j):
        return (s, lax.rem(c + j, dp))

    after = (lax.rem(s + 1, sp), c)
    before = (lax.rem(s + sp - 1, sp), c)

    def remote(src, dst, send, recv, to):
        return pltpu.make_async_remote_copy(
            src_ref=src, dst_ref=dst, send_sem=send, recv_sem=recv,
            device_id=to, device_id_type=pl.DeviceIdType.MESH)

    def lanes(i):
        if chunks == 1:
            return pl.ds(0, tw)
        return pl.ds(pl.multiple_of(i * tw, tw), tw)

    def place(i):
        if parts == 1:
            return 0, lanes(i)
        return i // per, pl.ds(pl.multiple_of(lax.rem(i, per) * tw, tw), tw)

    own_rows = pl.ds(pl.multiple_of(hi * tokens, tokens), tokens)
    own_depth = pl.ds(pl.multiple_of(lo * rows_w, rows_w), rows_w)
    barrier = pltpu.get_barrier_semaphore()
    peers = ([after, before] + [hi_peer(j) for j in range(1, b)]
             + [lo_peer(j) for j in range(1, a)] + [dp_peer(j) for j in range(1, dp)])
    for peer in peers:
        pl.semaphore_signal(barrier, inc=1, device_id=peer, device_id_type=pl.DeviceIdType.MESH)

    local = [pltpu.make_async_copy(val_in, val, loads.at[0]),
             pltpu.make_async_copy(gate_in, gate, loads.at[1]),
             pltpu.make_async_copy(cot.at[:, pl.ds(pl.multiple_of(hi * depth, 128), depth)],
                                   cotg.at[own_rows, :], loads.at[2])]
    for h in range(parts):
        local.append(pltpu.make_async_copy(w.at[:, h * wp:(h + 1) * wp], wg.at[h, own_depth, :], loads.at[3 + h]))
    for copy in local:
        copy.start()
    local[0].wait()
    local[1].wait()

    @pl.loop(0, chunks)
    def _(i):
        at = lanes(i)
        sig = jax.nn.sigmoid(gate[:, at].astype(F32))
        sgm[i] = sig
        mixed = (val[:, at].astype(F32) * sig).astype(BF16)
        hs1[:, at] = mixed[tokens - halo:]
        pin[i, halo:, :] = mixed.astype(F32)

    pl.semaphore_wait(barrier, len(peers))

    sends = []
    halo1 = remote(hs1, hr1, h1.at[0], h1.at[1], after)
    halo1.start()
    my_rows = pl.ds(pl.multiple_of(c * part_t, part_t), part_t)
    cot_in = []
    for j in range(1, b):
        other = lax.rem(hi + j, b)
        copy = remote(cot.at[my_rows, pl.ds(pl.multiple_of(other * depth, 128), depth)],
                      cotg.at[pl.ds(pl.multiple_of(hi * tokens + c * part_t, part_t), part_t), :],
                      cs.at[j - 1], cr.at[j - 1], hi_peer(j))
        copy.start()
        cot_in.append(copy)
    w_in = [[] for _ in range(parts)]
    for h in range(parts):
        for j in range(1, a):
            copy = remote(w.at[:, h * wp:(h + 1) * wp], wg.at[h, own_depth, :],
                          ws.at[h, j - 1], wr.at[h, j - 1], lo_peer(j))
            copy.start()
            w_in[h].append(copy)
    sends += [halo1] + cot_in + sum(w_in, [])

    halo1.wait_recv()
    keep_first = (s > 0).astype(F32)
    acc1[...] = jnp.zeros_like(acc1)
    acc2[...] = jnp.zeros_like(acc2)

    @pl.loop(0, chunks)
    def _(i):
        at = lanes(i)
        pin[i, :halo, :] = hr1[:, at].astype(F32) * keep_first
        total = jnp.zeros((tokens, tw), F32)
        for k in range(taps_n):
            total = total + taps[k:k + 1, at] * pin[i, base + k:base + k + tokens, :]
        rounded = total.astype(BF16).astype(F32)
        cbuf[i] = rounded
        acc1[...] += rounded
        acc2[...] += rounded * rounded

    def share(buf, got, send, recv):
        buf[0] = jnp.broadcast_to(jnp.sum(acc1[...], 1, keepdims=True), (tokens, tw))
        buf[1] = jnp.broadcast_to(jnp.sum(acc2[...], 1, keepdims=True), (tokens, tw))
        copies = []
        for j in range(1, dp):
            copy = remote(buf, got.at[j - 1], send.at[j - 1], recv.at[j - 1], dp_peer(j))
            copy.start()
            copies.append(copy)
        return copies

    def gathered(buf, got, copies):
        for copy in copies:
            copy.wait_recv()
        for j in range(1, dp):
            buf_sum = got[j - 1]
            acc1[...] = (buf[0] if j == 1 else acc1[...]) + buf_sum[0]
            acc2[...] = (buf[1] if j == 1 else acc2[...]) + buf_sum[1]

    first = share(ps1, pr1, p1s, p1r)
    gathered(ps1, pr1, first)
    sends += first
    mean = acc1[...] / channels
    inv[...] = lax.rsqrt(acc2[...] / channels - mean * mean + norm_floor)
    acc1[...] = mean

    @pl.loop(0, chunks)
    def _(i):
        at = lanes(i)
        normed = (cbuf[i] - acc1[...]) * inv[...]
        act = normed * gain[at][None, :]
        part, within = place(i)
        sig = jax.nn.sigmoid(act)
        swg[part, own_rows, within] = (act * sig).astype(BF16)
        nrm[i] = normed
        dact[i] = sig * (1.0 + act * (1.0 - sig))

    def sw_copy(step, up, source):
        rows = swg.at[:, pl.ds(pl.multiple_of(source * tokens, tokens), tokens), :]
        way = 0 if up else 1
        return remote(rows, rows, ss.at[way, step], sr.at[way, step], hi_peer(1 if up else b - 1))

    def sw_send(step, finish_it=False):
        for up in (True, False):
            source = hi - step if up else hi + step
            here = (source >= 0) & (hi + 1 < b) if up else (source < b) & (hi > 0)

            @pl.when(here)
            def _():
                copy = sw_copy(step, up, source)
                if finish_it:
                    copy.wait_send()
                else:
                    copy.start()

    def sw_take(step):
        for up in (True, False):
            source = hi - 1 - step if up else hi + 1 + step

            @pl.when(source >= 0 if up else source < b)
            def _():
                sw_copy(step, up, source).wait_recv()

    sw_send(0)

    forwards = []
    for j in range(1, b):
        cot_in[j - 1].wait_recv()
        origin = lax.rem(hi + b - j, b)
        rows = cotg.at[pl.ds(pl.multiple_of(origin * tokens + c * part_t, part_t), part_t), :]
        for d in range(1, dp):
            copy = remote(rows, rows, fs.at[j - 1, d - 1], fr.at[j - 1, d - 1], dp_peer(d))
            copy.start()
            forwards.append(copy)
    sends += forwards
    for copy in local[2:]:
        copy.wait()
    for copy in forwards:
        copy.wait_recv()

    def mix_copy(h, j):
        return remote(mixs.at[h, j - 1], mixr.at[h, j - 1], ms.at[h, j - 1], mr.at[h, j - 1], hi_peer(j))

    for step in range(b - 2):
        sw_take(step)
        sw_send(step + 1)
    for copy in sum(w_in, []):
        copy.wait_recv()
    short = jnp.minimum(hi, b - 1 - hi)
    longer = 1 - 2 * (hi > b - 1 - hi).astype(jnp.int32)

    @pl.loop(0, b - 1)
    def _(o):
        near = (o // 2 + 1) * (1 - 2 * lax.rem(o, 2))
        far = longer * (o - short + 1)
        move = jnp.where(o < 2 * short, near, far)
        j = lax.rem(move + b, b)
        other = hi + move
        block = cotg[pl.ds(pl.multiple_of(other * tokens, tokens), tokens), :]
        for h in range(parts):
            mixs[h, j - 1] = jnp.dot(block, wg[h], preferred_element_type=F32).astype(BF16)
            mix_copy(h, j).start()

    for h in range(parts):
        own_mix[h] = jnp.dot(cotg[own_rows, :], wg[h], preferred_element_type=F32)
    for q in range(a):
        cott[q * rows_w:(q + 1) * rows_w, :] = cotg[:, q * rows_w:(q + 1) * rows_w].T

    def gw_copy(h, j):
        return remote(gws.at[h, j - 1], gwr.at[h, j - 1], gs.at[h, j - 1], gr.at[h, j - 1], lo_peer(j))

    def gw_part(h):
        @pl.loop(1, a)
        def _(j):
            other = lax.rem(lo + j, a)
            block = cott[pl.ds(pl.multiple_of(other * rows_w, rows_w), rows_w), :]
            gws[h, j - 1] = jnp.dot(block, swg[h], preferred_element_type=F32).astype(BF16)
            gw_copy(h, j).start()

        own_gw[h] = jnp.dot(cott[own_depth, :], swg[h], preferred_element_type=F32)

    if b > 1:
        sw_take(b - 2)
    for h in range(max(parts - 1, 1)):
        gw_part(h)

    for h in range(parts):
        for j in range(1, b):
            mix_copy(h, j).wait_recv()
    acc1[...] = jnp.zeros_like(acc1)
    acc2[...] = jnp.zeros_like(acc2)
    red[...] = jnp.zeros_like(red)

    @pl.loop(0, chunks)
    def _(i):
        at = lanes(i)
        part, within = place(i)
        mix = own_mix[part, :, within]
        for j in range(1, b):
            mix = mix + mixr[part, j - 1, :, within].astype(F32)
        grad_act = mix * dact[i]
        normed = nrm[i]
        red[taps_n:taps_n + 1, at] = jnp.sum(grad_act * normed, 0, keepdims=True)
        grad_norm = grad_act * gain[at][None, :]
        cbuf[i] = grad_norm
        acc1[...] += grad_norm
        acc2[...] += grad_norm * normed

    second = share(ps2, pr2, p2s, p2r)
    gathered(ps2, pr2, second)
    sends += second
    acc1[...] = acc1[...] / channels
    acc2[...] = acc2[...] / channels

    @pl.loop(0, chunks)
    def _(i):
        at = lanes(i)
        rounded = (inv[...] * (cbuf[i] - acc1[...] - nrm[i] * acc2[...])).astype(BF16)
        hs2[:, at] = rounded[:halo]
        gcp[i, :tokens, :] = rounded.astype(F32)

    halo2 = remote(hs2, hr2, h2.at[0], h2.at[1], before)
    halo2.start()
    sends.append(halo2)

    @pl.loop(0, chunks)
    def _(i):
        at = lanes(i)
        grad = gcp[i, :tokens, :]
        for k in range(taps_n):
            red[k:k + 1, at] = jnp.sum(grad * pin[i, base + k:base + k + tokens, :], 0, keepdims=True)

    stage1 = []
    for j in range(1, a):
        other = lax.rem(lo + j, a)
        copy = remote(red.at[pl.ds(pl.multiple_of(other * rows_r, 8), rows_r), :], r1.at[j - 1],
                      t1s.at[j - 1], t1r.at[j - 1], lo_peer(j))
        copy.start()
        stage1.append(copy)
    sends += stage1
    if parts > 1:
        gw_part(parts - 1)

    halo2.wait_recv()
    keep_last = (s < sp - 1).astype(F32)

    @pl.loop(0, chunks)
    def _(i):
        at = lanes(i)
        gcp[i, tokens:, :] = hr2[:, at].astype(F32) * keep_last
        total = jnp.zeros((tokens, tw), F32)
        for k in range(taps_n):
            back = taps_n - 1 - k
            total = total + taps[k:k + 1, at] * gcp[i, back:back + tokens, :]
        grad = total.astype(BF16).astype(F32)
        sig = sgm[i]
        gv[:, at] = (grad * sig).astype(BF16)
        gg[:, at] = (grad * val[:, at].astype(F32) * sig * (1.0 - sig)).astype(BF16)

    for copy in stage1:
        copy.wait_recv()
    mine = red[pl.ds(pl.multiple_of(lo * rows_r, 8), rows_r), :]
    for j in range(1, a):
        mine = mine + r1[j - 1]
    r2[hi] = mine
    stage2 = []
    for j in range(1, b):
        copy = remote(r2.at[hi], r2.at[hi], t2s.at[j - 1], t2r.at[j - 1], hi_peer(j))
        copy.start()
        stage2.append(copy)
    sends += stage2
    for copy in stage2:
        copy.wait_recv()
    summed = r2[0]
    for j in range(1, b):
        summed = summed + r2[j]
    my_red = pl.ds(pl.multiple_of(lo * rows_r, 8), rows_r)
    gts[my_red, :] = summed
    stage3 = []
    for j in range(1, a):
        copy = remote(gts.at[my_red, :], gts.at[my_red, :], t3s.at[j - 1], t3r.at[j - 1], lo_peer(j))
        copy.start()
        stage3.append(copy)
    sends += stage3

    for h in range(parts):
        for j in range(1, a):
            gw_copy(h, j).wait_recv()
        total = own_gw[h]
        for j in range(1, a):
            total = total + gwr[h, j - 1].astype(F32)
        gw[:, h * wp:(h + 1) * wp] = total

    for copy in stage3:
        copy.wait_recv()
    gt[...] = gts[...]

    for copy in sends:
        copy.wait_send()
    for step in range(b - 1):
        sw_send(step, True)
    for h in range(parts):
        for j in range(1, b):
            mix_copy(h, j).wait_send()
        for j in range(1, a):
            gw_copy(h, j).wait_send()


def finish(gv, gg, gw, gt, out_gv, out_gg, out_gw, out_taps, out_gain):
    out_gv[...] = gv[...]
    out_gg[...] = gg[...]
    out_gw[...] = gw[...]
    taps_n = out_taps.shape[0]
    out_taps[...] = gt[:taps_n]
    out_gain[...] = gt[taps_n]


def body(sp, dp, val, gate, cot, w, taps, gain):
    a = LOW if sp % LOW == 0 else 1
    b = sp // a
    tokens, width = val.shape
    rows_w = w.shape[0]
    model = cot.shape[1]
    depth = model // b
    taps_n = taps.shape[0]
    tw = 128 if width % 128 == 0 else width
    chunks = width // tw
    halo = -(-(taps_n - 1) // 16) * 16
    rows = -(-(taps_n + 1) // (8 * a)) * 8 * a
    parts = 3 if chunks % 3 == 0 else 2 if chunks % 2 == 0 else 1
    wp = width // parts
    vm, dma = pltpu.VMEM, pltpu.SemaphoreType.DMA
    scratch = [
        vm((tokens, width), BF16),
        vm((tokens, width), BF16),
        dma((3 + parts,)),
        vm((depth, b * tokens), BF16),
        vm((chunks, tokens + halo, tw), F32),
        vm((chunks, tokens + halo, tw), F32),
        vm((chunks, tokens, tw), F32),
        vm((chunks, tokens, tw), F32),
        vm((chunks, tokens, tw), F32),
        vm((chunks, tokens, tw), F32),
        vm((tokens, tw), F32),
        vm((tokens, tw), F32),
        vm((tokens, tw), F32),
        vm((halo, width), BF16),
        vm((halo, width), BF16),
        vm((halo, width), BF16),
        vm((halo, width), BF16),
        vm((b * tokens, depth), BF16),
        vm((parts, depth, wp), BF16),
        vm((parts, b * tokens, wp), BF16),
        vm((parts, tokens, wp), F32),
        vm((parts, b - 1, tokens, wp), BF16),
        vm((parts, b - 1, tokens, wp), BF16),
        vm((parts, rows_w, wp), F32),
        vm((parts, a - 1, rows_w, wp), BF16),
        vm((parts, a - 1, rows_w, wp), BF16),
        vm((2, tokens, tw), F32),
        vm((dp - 1, 2, tokens, tw), F32),
        vm((2, tokens, tw), F32),
        vm((dp - 1, 2, tokens, tw), F32),
        vm((rows, width), F32),
        vm((a - 1, rows // a, width), F32),
        vm((b, rows // a, width), F32),
        vm((rows, width), F32),
        dma((2,)), dma((2,)),
        dma((b - 1,)), dma((b - 1,)),
        dma((b - 1, dp - 1)), dma((b - 1, dp - 1)),
        dma((parts, a - 1)), dma((parts, a - 1)),
        dma((dp - 1,)), dma((dp - 1,)), dma((dp - 1,)), dma((dp - 1,)),
        dma((2, b - 1)), dma((2, b - 1)),
        dma((parts, b - 1)), dma((parts, b - 1)),
        dma((parts, a - 1)), dma((parts, a - 1)),
        dma((a - 1,)), dma((a - 1,)),
        dma((b - 1,)), dma((b - 1,)),
        dma((a - 1,)), dma((a - 1,)),
    ]
    spec = pl.BlockSpec(memory_space=pltpu.VMEM)
    anywhere = pl.BlockSpec(memory_space=pl.ANY)
    results = pl.pallas_call(
        functools.partial(kernel, (a, b, dp)),
        out_shape=(
            jax.ShapeDtypeStruct((tokens, width), BF16),
            jax.ShapeDtypeStruct((tokens, width), BF16),
            jax.ShapeDtypeStruct((rows_w, width), F32),
            jax.ShapeDtypeStruct((rows, width), F32),
        ),
        in_specs=[anywhere] * 4 + [spec] * 2,
        out_specs=(spec,) * 4,
        scratch_shapes=scratch,
        compiler_params=pltpu.CompilerParams(
            collective_id=0, has_side_effects=True, vmem_limit_bytes=56 * 1024 * 1024),
    )(val, gate, cot, w, taps, gain)
    return pl.pallas_call(
        finish,
        out_shape=(
            jax.ShapeDtypeStruct((tokens, width), BF16),
            jax.ShapeDtypeStruct((tokens, width), BF16),
            jax.ShapeDtypeStruct((rows_w, width), F32),
            jax.ShapeDtypeStruct((taps_n, width), F32),
            jax.ShapeDtypeStruct((width,), F32),
        ),
        in_specs=[spec] * 4,
        out_specs=(spec,) * 5,
    )(*results)


def solution(mesh):
    in_specs = (P("sp", "dp"), P("sp", "dp"), P("sp", None), P("sp", "dp"), P(None, "dp"), P("dp"))
    out_specs = (P("sp", "dp"), P("sp", "dp"), P("sp", "dp"), P(None, "dp"), P("dp"))
    run = functools.partial(body, mesh.shape["sp"], mesh.shape["dp"])
    return jax.shard_map(run, mesh=mesh, in_specs=in_specs, out_specs=out_specs, check_vma=False)
```
